512 devices in a mesh: sp: 64 (over z, y), tp: 8 (over x, core).
Axes of the slice: x: 4, y: 8, z: 8, core: 2. Of those that a mesh axis runs over, the one named last changes fastest.
Arguments:
- residual: bfloat16 [12288, 2048], P(('sp', 'tp')), may hold values from -6 to 6
- queries_narrow: bfloat16 [12288, 512], P('sp', 'tp'), may hold values from -24 to 24
- keys_narrow: bfloat16 [12288, 512], P('sp', 'tp'), may hold values from -24 to 24
- values_narrow: bfloat16 [12288, 512], P('sp', 'tp'), may hold values from -6 to 6
- queries_broad: bfloat16 [12288, 512], P('sp', 'tp'), may hold values from -24 to 24
- keys_broad: bfloat16 [12288, 512], P('sp', 'tp'), may hold values from -24 to 24
- values_broad: bfloat16 [12288, 512], P('sp', 'tp'), may hold values from -6 to 6
- gates_narrow: float32 [12288, 16], P('sp', 'tp'), may hold values from -12288 to 0, as said below
- gates_broad: float32 [12288, 8], P('sp', 'tp'), may hold values from -12288 to 0, as said below
- project_narrow: bfloat16 [512, 2048], P('tp'), may hold values from -0.5 to 0.5
- project_broad: bfloat16 [512, 2048], P('tp'), may hold values from -0.5 to 0.5
- norm_gain: float32 [2048], replicated, may hold values from 0.1 to 1.9
- up_weight: bfloat16 [2048, 8192], P('sp', 'tp'), may hold values from -0.125 to 0.125
- down_weight: bfloat16 [8192, 2048], P('tp', 'sp'), may hold values from -0.0625 to 0.0625
Outputs:
- layer_out: bfloat16 [12288, 2048], P(('sp', 'tp'))
The draws below stay inside these ranges and needn't reach their ends.
Inputs may be any that keep to these rules, and one draw needn't show every extreme that they name: `gates_narrow`: each head's cumulative log gate never rises from one position to the next. `gates_broad`: each head's cumulative log gate never rises from one position to the next.
All inputs are finite; a program needn't handle non-finite values.
Results may differ from the reference program's by a relative error of at most 0.018.
Values may be sent and summed in bfloat16 or wider, within the bound.
A program may use at most 128 MiB of HBM per device.

```python
import jax
import jax.numpy as jnp
from jax import lax

D = 2048
FF = 8192
A_HEADS = 16
A_DIM = 32
B_HEADS = 8
B_DIM = 64
TOK_DEV = 192
CONTEXT_LENGTH = 12288


def paired_rows(key, width):
    key_query, key_keys = jax.random.split(key, 2)
    queries = jax.random.normal(key_query, (CONTEXT_LENGTH, width), jnp.float32)
    keys = jax.random.normal(key_keys, (CONTEXT_LENGTH, width), jnp.float32)
    return (queries.astype(jnp.bfloat16), keys.astype(jnp.bfloat16))


def draw_queries_narrow(key, part):
    return paired_rows(jax.random.fold_in(key, 11), A_HEADS * A_DIM)[0]


def draw_keys_narrow(key, part):
    return paired_rows(jax.random.fold_in(key, 11), A_HEADS * A_DIM)[1]


def draw_queries_broad(key, part):
    return paired_rows(jax.random.fold_in(key, 12), B_HEADS * B_DIM)[0]


def draw_keys_broad(key, part):
    return paired_rows(jax.random.fold_in(key, 12), B_HEADS * B_DIM)[1]


def forget_gates(key, heads):
    category_seed, quick_decay_seed, gradual_decay_seed, tile_seed, sample_seed, spike_seed, quantity_seed = jax.random.split(key, 7)
    slow_share = 0.5
    slow = jax.random.uniform(category_seed, (heads,), jnp.float32) < slow_share
    fast_rate = 1.0 / jax.random.uniform(quick_decay_seed, (heads,), jnp.float32, 30.0, 50.0)
    slow_rate = jax.random.uniform(gradual_decay_seed, (heads,), jnp.float32, 0.5, 1.0) / CONTEXT_LENGTH
    rate = jnp.where(slow, slow_rate, fast_rate)
    blocks = CONTEXT_LENGTH // TOK_DEV
    block_factor = jnp.exp(jax.random.uniform(tile_seed, (blocks,), jnp.float32, -0.7, 0.7))
    block_factor = jnp.repeat(block_factor, TOK_DEV)
    data_part = jnp.exp(jax.random.uniform(sample_seed, (CONTEXT_LENGTH, heads), jnp.float32, -1.2, 1.1))
    forget_log_factor = -rate[None, :] * block_factor[:, None] * data_part
    position_spike = jax.random.uniform(spike_seed, (CONTEXT_LENGTH, 1), jnp.float32) < 2.0 / CONTEXT_LENGTH
    position_quantity = jax.random.uniform(quantity_seed, (CONTEXT_LENGTH, heads), jnp.float32, 0.22, 0.69)
    forget_log_factor = forget_log_factor - jnp.where(position_spike, position_quantity, 0.0)
    return jnp.cumsum(forget_log_factor, axis=0)


def draw_gates_narrow(key, part):
    return forget_gates(jax.random.fold_in(key, 21), A_HEADS)


def draw_gates_broad(key, part):
    return forget_gates(jax.random.fold_in(key, 22), B_HEADS)


def block_scale(key, shape, cuts, low, high):
    gain, own = 1.0, jax.random.fold_in(key, 6)
    for dim, blocks in cuts:
        steps = jnp.exp(jax.random.uniform(jax.random.fold_in(own, dim), (blocks,), jnp.float32, low / len(cuts), high / len(cuts)))
        gain = gain * jnp.repeat(steps, shape[dim] // blocks).reshape([-1 if axis == dim else 1 for axis in range(len(shape))])
    return gain


def bell_draw(own_key, extent, spread, limit, cuts=(), kind=jnp.bfloat16):
    array = spread * jax.random.normal(own_key, extent, jnp.float32)
    if cuts:
        array = array * block_scale(own_key, extent, cuts, -0.22, 0.18)
    return jnp.clip(array, -limit, limit).astype(kind)


def setup_inputs(seed: int = 0) -> dict:
    streams_of = jax.random.split(jax.random.key(seed), 15)
    return {
        "residual": bell_draw(streams_of[0], (CONTEXT_LENGTH, D), 1.0, 6.0, ((0, 512),)),
        "queries_narrow": draw_queries_narrow(jax.random.fold_in(streams_of[14], 71), 0),
        "keys_narrow": draw_keys_narrow(jax.random.fold_in(streams_of[14], 71), 0),
        "values_narrow": bell_draw(streams_of[3], (CONTEXT_LENGTH, A_HEADS * A_DIM), 1.0, 6.0, ((0, 64), (1, 8))),
        "queries_broad": draw_queries_broad(jax.random.fold_in(streams_of[14], 71), 0),
        "keys_broad": draw_keys_broad(jax.random.fold_in(streams_of[14], 71), 0),
        "values_broad": bell_draw(streams_of[6], (CONTEXT_LENGTH, B_HEADS * B_DIM), 1.0, 6.0, ((0, 64), (1, 8))),
        "gates_narrow": draw_gates_narrow(jax.random.fold_in(streams_of[14], 71), 0),
        "gates_broad": draw_gates_broad(jax.random.fold_in(streams_of[14], 71), 0),
        "project_narrow": bell_draw(streams_of[9], (A_HEADS * A_DIM, D), ((A_HEADS * A_DIM + B_HEADS * B_DIM) // 8) ** -0.5, 0.5, ((0, 8),)),
        "project_broad": bell_draw(streams_of[10], (B_HEADS * B_DIM, D), ((A_HEADS * A_DIM + B_HEADS * B_DIM) // 8) ** -0.5, 0.5, ((0, 8),)),
        "norm_gain": jnp.clip(1.0 + 0.18 * jax.random.normal(streams_of[11], (D,), jnp.float32), 0.1, 1.9),
        "up_weight": bell_draw(streams_of[12], (D, FF), D ** -0.5, 0.125, ((0, 64), (1, 8))),
        "down_weight": bell_draw(streams_of[13], (FF, D), FF ** -0.5, 0.0625, ((0, 8), (1, 64))),
    }


def group_attention(queries, keys, values, gates, head_size):
    total_rows = queries.shape[0]
    heads = queries.shape[1] // head_size
    block = min(512, total_rows)
    blocks = total_rows // block
    query_blocks = queries.astype(jnp.float32).reshape(blocks, block, heads, head_size)
    gate_blocks = gates.reshape(blocks, block, heads)
    key_heads = keys.astype(jnp.float32).reshape(total_rows, heads, head_size)
    value_heads = values.astype(jnp.float32).reshape(total_rows, heads, head_size)
    key_pos = jnp.arange(total_rows, dtype=jnp.int32)

    def one_block(inputs):
        index, query_block, gate_block = inputs
        scores = jnp.einsum('qhd,khd->hqk', query_block, key_heads) * head_size ** (-0.5)
        scores = scores + gate_block.T[:, :, None] - gates.T[:, None, :]
        query_pos = index * block + jnp.arange(block, dtype=jnp.int32)
        allowed = key_pos[None, :] <= query_pos[:, None]
        scores = jnp.where(allowed[None], scores, -jnp.inf)
        peak = lax.optimization_barrier(jnp.max(scores, axis=-1, keepdims=True))
        weights = jnp.exp(scores - peak)
        denom = lax.optimization_barrier(jnp.sum(weights, axis=-1))
        summed = jnp.einsum('hqk,khd->hqd', weights.astype(jnp.bfloat16).astype(jnp.float32), value_heads)
        result = summed / denom[..., None]
        return result.transpose(1, 0, 2).reshape(block, heads * head_size)
    output = lax.map(one_block, (jnp.arange(blocks, dtype=jnp.int32), query_blocks, gate_blocks))
    return output.reshape(total_rows, heads * head_size).astype(jnp.bfloat16)

def reference(residual, queries_narrow, keys_narrow, values_narrow, queries_broad, keys_broad, values_broad, gates_narrow, gates_broad, project_narrow, project_broad, norm_gain, up_weight, down_weight):
    attended_narrow = group_attention(queries_narrow, keys_narrow, values_narrow, gates_narrow, A_DIM)
    attended_broad = group_attention(queries_broad, keys_broad, values_broad, gates_broad, B_DIM)
    projected = jnp.dot(attended_narrow, project_narrow, preferred_element_type=jnp.float32)
    projected = projected + jnp.dot(attended_broad, project_broad, preferred_element_type=jnp.float32)
    mixed = (residual.astype(jnp.float32) + projected).astype(jnp.bfloat16)
    mixed_wide = mixed.astype(jnp.float32)
    scale = lax.rsqrt(lax.optimization_barrier(jnp.mean(mixed_wide * mixed_wide, axis=-1, keepdims=True)) + 1e-06)
    normed = (mixed_wide * scale * norm_gain.astype(jnp.float32)).astype(jnp.bfloat16)
    hidden = jnp.square(jax.nn.relu(jnp.dot(normed, up_weight, preferred_element_type=jnp.float32))).astype(jnp.bfloat16)
    return (mixed_wide + jnp.dot(hidden, down_weight, preferred_element_type=jnp.float32)).astype(jnp.bfloat16)
```

```python
import functools

import jax
import jax.numpy as jnp
from jax import lax
from jax.experimental import pallas as pl
from jax.experimental.pallas import tpu as pltpu
from jax.sharding import PartitionSpec as P

A_DIM = 32
B_DIM = 64
LOG2E = 1.4426950408889634
FAR = 1e30
MESH = pl.DeviceIdType.MESH
BF = jnp.bfloat16
F32 = jnp.float32


def split_sp(mesh):
    size = mesh.shape["sp"]
    ny = 1
    while ny * ny < size:
        ny *= 2
    return size // ny, ny


def rcopy(src, dst, send, recv, device):
    return pltpu.make_async_remote_copy(
        src_ref=src,
        dst_ref=dst,
        send_sem=send,
        recv_sem=recv,
        device_id=device,
        device_id_type=MESH,
    )


def nt_dot(a, b):
    return lax.dot_general(a, b, (((1,), (1,)), ((), ())), preferred_element_type=F32)


def head_mask(shape):
    lane = lax.broadcasted_iota(jnp.int32, shape, 1)
    return (lane < A_DIM, (lane >= A_DIM) & (lane < 2 * A_DIM), lane >= 2 * A_DIM)


SCALES = (A_DIM**-0.5 * LOG2E, A_DIM**-0.5 * LOG2E, B_DIM**-0.5 * LOG2E)


class Tp:
    def __init__(self, nx, buf, xs, xr, ds, dr):
        self.nx, self.buf, self.xs, self.xr, self.ds, self.dr = nx, buf, xs, xr, ds, dr
        self.sp, self.tp = lax.axis_index("sp"), lax.axis_index("tp")
        self.x, self.c = self.tp // 2, self.tp % 2

    def across(self, i):
        to = ((self.x + i) % self.nx) * 2 + self.c
        return rcopy(
            self.buf.at[self.tp], self.buf.at[self.tp], self.xs.at[i - 1], self.xr.at[i - 1], (self.sp, to)
        )

    def arrived(self, i):
        return ((self.x - i + self.nx) % self.nx) * 2 + self.c

    def beside(self, i):
        src = self.arrived(i)
        return rcopy(
            self.buf.at[src], self.buf.at[src], self.ds.at[i], self.dr.at[i], (self.sp, self.x * 2 + 1 - self.c)
        )

    def start(self):
        for i in range(1, self.nx):
            self.across(i).start()
        self.beside(0).start()

    def forward(self, i):
        self.across(i).wait_recv()
        self.beside(i).start()

    def finish(self):
        for i in range(self.nx):
            self.beside(i).wait_recv()
        for i in range(1, self.nx):
            self.across(i).wait_send()
        for i in range(self.nx):
            self.beside(i).wait_send()


def front(
    nz,
    ny,
    nt,
    qn,
    qb,
    kn,
    kb,
    vn,
    vb,
    gn,
    gb,
    pn,
    pb,
    res,
    gain,
    mixed_out,
    feat_out,
    qbuf,
    kbuf,
    vbuf,
    gbuf,
    gk,
    pw,
    osend,
    lsend,
    orecv,
    lrecv,
    asend,
    arecv,
    feat,
    pw_in,
    q_s,
    q_r,
    kv_s,
    kv_r,
    pw_xs,
    pw_xr,
    pw_ds,
    pw_dr,
    p_s,
    p_r,
    a_s,
    a_r,
    f_xs,
    f_xr,
    f_ds,
    f_dr,
):
    nx = nt // 2
    sp, tp = lax.axis_index("sp"), lax.axis_index("tp")
    z, y = sp // ny, sp % ny
    tok = qn.shape[0]
    rows = tok // nt
    keys = nz * tok
    d = res.shape[1]

    qbuf[y, 0:tok, 0:64] = qn[...]
    qbuf[y, 0:tok, 64:128] = qb[...]
    kbuf[0, :, 0:64] = kn[...]
    kbuf[0, :, 64:128] = kb[...]
    vbuf[0, :, 0:64] = vn[...]
    vbuf[0, :, 64:128] = vb[...]
    for r in range(nz):
        vbuf[r, :, 128:256] = jnp.ones((tok, 128), BF)
    lane = lax.broadcasted_iota(jnp.int32, (tok, 128), 1)
    gates = jnp.where(
        lane == 0,
        gn[:, 0:1],
        jnp.where(lane == 1, gn[:, 1:2], jnp.where(lane == 2, gb[:, 0:1], 0.0)),
    )
    qbuf[y, tok : tok + 16, :] = gates[0:16].astype(BF)
    gbuf[0, :, 0:tok] = jnp.transpose(gates)[0:8]
    gbuf[0, :, tok:256] = jnp.zeros((8, 256 - tok), F32)

    load_n = pltpu.make_async_copy(pn, pw.at[tp, 0:64], pw_in.at[0])
    load_b = pltpu.make_async_copy(pb, pw.at[tp, 64:128], pw_in.at[1])
    load_n.start()
    load_b.start()

    barrier = pltpu.get_barrier_semaphore()
    peers = [(z * ny + (y + i) % ny, tp) for i in range(1, ny)]
    up_z, down_z = ((z + 1) % nz) * ny + y, ((z + nz - 1) % nz) * ny + y
    peers += [(up_z, tp), (down_z, tp)]
    peers += [(sp, (tp + i) % nt) for i in range(1, nt)]
    for peer in peers:
        pl.semaphore_signal(barrier, inc=1, device_id=peer, device_id_type=MESH)
    pl.semaphore_wait(barrier, len(peers))

    def ring(slot, src, to):
        return [
            rcopy(kbuf.at[src], kbuf.at[slot], kv_s.at[0, slot - 1], kv_r.at[0, slot - 1], (to, tp)),
            rcopy(
                vbuf.at[src, :, 0:128],
                vbuf.at[slot, :, 0:128],
                kv_s.at[1, slot - 1],
                kv_r.at[1, slot - 1],
                (to, tp),
            ),
            rcopy(gbuf.at[src], gbuf.at[slot], kv_s.at[2, slot - 1], kv_r.at[2, slot - 1], (to, tp)),
        ]

    rights = nz // 2
    lefts = nz - 1 - rights
    steps = [ring(s, s - 1, up_z) for s in range(1, rights + 1)]
    steps_left = [ring(nz - s, (nz - s + 1) % nz, down_z) for s in range(1, lefts + 1)]

    q_sends = [
        rcopy(
            qbuf.at[y], qbuf.at[y], q_s.at[i - 1], q_r.at[i - 1], (z * ny + (y + i) % ny, tp)
        )
        for i in range(1, ny)
    ]
    for c in steps[0]:
        c.start()
    for chain in steps_left[0:1]:
        for c in chain:
            c.start()
    for c in q_sends:
        c.start()
    load_n.wait()
    load_b.wait()
    share = Tp(nx, pw, pw_xs, pw_xr, pw_ds, pw_dr)
    share.start()

    for s in range(1, rights + 1):
        for c in steps[s - 1]:
            c.wait_recv()
        if s < rights:
            for c in steps[s]:
                c.start()
        if s <= lefts:
            for c in steps_left[s - 1]:
                c.wait_recv()
            if s < lefts:
                for c in steps_left[s]:
                    c.start()

    for r in range(nz):
        gk[:, r * tok : (r + 1) * tok] = jnp.where(r <= z, gbuf[r, :, 0:tok], FAR)

    col = lax.broadcasted_iota(jnp.int32, (1, keys), 1)

    def block(src, own, out_o, out_l):
        q = qbuf[src, 0:tok, :]
        masks = head_mask((tok, 128))
        k = kbuf[...].reshape(keys, 128)
        v = vbuf[...].reshape(keys, 256)
        outs, lses = [], []
        for h in range(3):
            s = nt_dot(jnp.where(masks[h], q, jnp.zeros_like(q)), k)
            ref = qbuf[src, tok : tok + 16, :][0:1, h : h + 1].astype(F32)
            bias = (ref - gk[h : h + 1, :]) * LOG2E
            if not own:
                bias = jnp.where((col < tok) & (y > src), -FAR, bias)
            s = s * SCALES[h] + bias
            if own:
                wide = min(keys, 256)
                first = s[:, 0:wide]
                at = lax.broadcasted_iota(jnp.int32, first.shape, 1)
                row = lax.broadcasted_iota(jnp.int32, first.shape, 0)
                first = jnp.where((at < tok) & (at > row), -FAR, first)
                s = jnp.concatenate([first, s[:, wide:]], axis=1) if keys > wide else first
            m = jnp.max(s, axis=1, keepdims=True)
            w = jnp.exp2(s - m).astype(BF)
            o = jnp.dot(w, v, preferred_element_type=F32)
            total = o[:, 128:256]
            outs.append(o[:, 0:128] / total)
            lses.append(m + jnp.log2(total))
        out_o[...] = jnp.where(masks[0], outs[0], jnp.where(masks[1], outs[1], outs[2])).astype(BF)
        lse = jnp.where(lane == 0, lses[0], jnp.where(lane == 1, lses[1], lses[2]))
        out_l[:, 0:tok] = jnp.transpose(lse)[0:8]

    def give(i):
        src = (y + ny - i) % ny
        to = (z * ny + src, tp)
        return [
            rcopy(osend.at[i - 1], orecv.at[y], p_s.at[0, i - 1], p_r.at[0, i - 1], to),
            rcopy(lsend.at[i - 1], lrecv.at[y], p_s.at[1, i - 1], p_r.at[1, i - 1], to),
        ]

    def one(i, carry):
        src = (y + ny - i) % ny
        rcopy(qbuf.at[y], qbuf.at[src], q_s.at[i - 1], q_r.at[i - 1], (z * ny + src, tp)).wait_recv()
        block(src, False, osend.at[i - 1], lsend.at[i - 1])
        for c in give(i):
            c.start()
        return carry

    lax.fori_loop(1, ny, one, 0)
    block(y, True, orecv.at[y], lrecv.at[y])
    for i in range(1, nx):
        share.forward(i)
    for i in range(1, ny):
        for c in give(i):
            c.wait_recv()

    lse = [lrecv[j, :, 0:tok] for j in range(ny)]
    peak = functools.reduce(jnp.maximum, lse)
    parts = [jnp.exp2(a - peak) for a in lse]
    inv = 1.0 / functools.reduce(jnp.add, parts)
    share_t = jnp.transpose(jnp.concatenate([a * inv for a in parts], axis=0))
    masks = head_mask((tok, 128))
    att = jnp.zeros((tok, 128), F32)
    for j in range(ny):
        f = [share_t[:, 8 * j + h : 8 * j + h + 1] for h in range(3)]
        factor = jnp.where(masks[0], f[0], jnp.where(masks[1], f[1], f[2]))
        att = att + factor * orecv[j].astype(F32)
    for t in range(nt):
        asend[t] = att[t * rows : (t + 1) * rows].astype(BF)

    def hand(i):
        to = (tp + i) % nt
        return rcopy(asend.at[to], arecv.at[tp], a_s.at[i - 1], a_r.at[i - 1], (sp, to))

    for i in range(1, nt):
        hand(i).start()
    arecv[tp] = asend[tp]
    share.finish()
    for i in range(1, nt):
        hand(i).wait_recv()

    full = jnp.concatenate([arecv[t] for t in range(nt)], axis=1)
    projected = jnp.dot(full, pw[...].reshape(nt * 128, d), preferred_element_type=F32)
    mixed = (res[...].astype(F32) + projected).astype(BF)
    mixed_out[...] = mixed
    wide = mixed.astype(F32)
    scale = lax.rsqrt(jnp.mean(wide * wide, axis=-1, keepdims=True) + 1e-6)
    feat[tp] = (wide * scale * gain[...]).astype(BF)

    spread = Tp(nx, feat, f_xs, f_xr, f_ds, f_dr)
    spread.start()
    for i in range(1, nx):
        spread.forward(i)
    spread.finish()
    feat_out[...] = feat[...]

    for chain in steps + steps_left:
        for c in chain:
            c.wait_send()
    for c in q_sends:
        c.wait_send()
    for i in range(1, ny):
        for c in give(i):
            c.wait_send()
    for i in range(1, nt):
        hand(i).wait_send()


def ffn(nt, feat, mixed, w, out, up, down, part, pair, psum, got, w_in, pair_s, pair_r, g_s, g_r):
    nx = nt // 2
    sp, tp = lax.axis_index("sp"), lax.axis_index("tp")
    x, c = tp // 2, tp % 2
    rows, d = mixed.shape
    nsp, band = up.shape[0], up.shape[1]
    load_up = pltpu.make_async_copy(w.at[:, 0:band], up, w_in.at[0])
    load_down = pltpu.make_async_copy(w.at[:, band : 2 * band], down, w_in.at[1])
    load_up.start()
    load_down.start()

    barrier = pltpu.get_barrier_semaphore()
    beside = (sp, x * 2 + 1 - c)
    peers = [beside] + [(sp, ((x + i) % nx) * 2 + c) for i in range(1, nx)]
    for peer in peers:
        pl.semaphore_signal(barrier, inc=1, device_id=peer, device_id_type=MESH)
    pl.semaphore_wait(barrier, len(peers))

    load_up.wait()
    f = feat[...].reshape(nt * rows, d)
    ff = up.shape[2]
    h = jnp.dot(f, up[...].reshape(nsp * band, ff), preferred_element_type=F32)
    h = jnp.square(jnp.maximum(h, 0.0)).astype(BF)
    load_down.wait()
    total = nt_dot(h, down[...].reshape(nsp * band, ff))
    for t in range(nt):
        block = total[t * rows : (t + 1) * rows]

        @pl.when(c == t % 2)
        def _():
            part[t // 2] = block

        @pl.when(c != t % 2)
        def _():
            psum[t // 2] = block.astype(BF)

    swap = rcopy(psum, pair, pair_s, pair_r, beside)
    swap.start()
    swap.wait()

    def give(i):
        to = (x + i) % nx
        return rcopy(psum.at[to], got.at[i - 1], g_s.at[i - 1], g_r.at[i - 1], (sp, to * 2 + c))

    for i in range(1, nx):
        to = (x + i) % nx
        psum[to] = (part[to] + pair[to].astype(F32)).astype(BF)
        give(i).start()
    acc = mixed[...].astype(F32) + (part[x] + pair[x].astype(F32))
    for i in range(1, nx):
        give(i).wait_recv()
        acc = acc + got[i - 1].astype(F32)
    out[...] = acc.astype(BF)
    for i in range(1, nx):
        give(i).wait_send()


def local(nz, ny, nt, *args):
    res, qn, kn, vn, qb, kb, vb, gn, gb, pn, pb, gain, up, down = args
    tok = qn.shape[0]
    rows, d = res.shape
    nx = nt // 2
    band, ff = up.shape
    nsp = nz * ny
    w = jnp.concatenate([up, down.T], axis=0)
    w = lax.all_gather(w, "sp", axis=0, tiled=True).reshape(nsp, 2 * band, ff)

    dma = pltpu.SemaphoreType.DMA
    vmem = pl.BlockSpec(memory_space=pltpu.VMEM)
    anyw = pl.BlockSpec(memory_space=pl.ANY)
    mixed, feat = pl.pallas_call(
        functools.partial(front, nz, ny, nt),
        out_shape=(
            jax.ShapeDtypeStruct((rows, d), BF),
            jax.ShapeDtypeStruct((nt, rows, d), BF),
        ),
        in_specs=[vmem] * 8 + [anyw] * 2 + [vmem] * 2,
        out_specs=(vmem, vmem),
        scratch_shapes=[
            pltpu.VMEM((ny, tok + 16, 128), BF),
            pltpu.VMEM((nz, tok, 128), BF),
            pltpu.VMEM((nz, tok, 256), BF),
            pltpu.VMEM((nz, 8, 256), F32),
            pltpu.VMEM((8, nz * tok), F32),
            pltpu.VMEM((nt, 128, d), BF),
            pltpu.VMEM((ny - 1, tok, 128), BF),
            pltpu.VMEM((ny - 1, 8, 256), F32),
            pltpu.VMEM((ny, tok, 128), BF),
            pltpu.VMEM((ny, 8, 256), F32),
            pltpu.VMEM((nt, rows, 128), BF),
            pltpu.VMEM((nt, rows, 128), BF),
            pltpu.VMEM((nt, rows, d), BF),
            dma((2,)),
            dma((ny - 1,)),
            dma((ny - 1,)),
            dma((3, nz - 1)),
            dma((3, nz - 1)),
            dma((nx - 1,)),
            dma((nx - 1,)),
            dma((nx,)),
            dma((nx,)),
            dma((2, ny - 1)),
            dma((2, ny - 1)),
            dma((nt - 1,)),
            dma((nt - 1,)),
            dma((nx - 1,)),
            dma((nx - 1,)),
            dma((nx,)),
            dma((nx,)),
        ],
        compiler_params=pltpu.CompilerParams(
            collective_id=0, has_side_effects=True, vmem_limit_bytes=48 * 1024 * 1024
        ),
        cost_estimate=pl.CostEstimate(
            flops=8_000_000_000, bytes_accessed=60_000_000, transcendentals=7_000_000
        ),
        name="front",
    )(qn, qb, kn, kb, vn, vb, gn, gb, pn, pb, res, gain.reshape(1, d))

    return pl.pallas_call(
        functools.partial(ffn, nt),
        out_shape=jax.ShapeDtypeStruct((rows, d), BF),
        in_specs=[vmem, vmem, anyw],
        out_specs=vmem,
        scratch_shapes=[
            pltpu.VMEM((nsp, band, ff), BF),
            pltpu.VMEM((nsp, band, ff), BF),
            pltpu.VMEM((nx, rows, d), F32),
            pltpu.VMEM((nx, rows, d), BF),
            pltpu.VMEM((nx, rows, d), BF),
            pltpu.VMEM((nx - 1, rows, d), BF),
            dma((2,)),
            dma,
            dma,
            dma((nx - 1,)),
            dma((nx - 1,)),
        ],
        compiler_params=pltpu.CompilerParams(
            collective_id=1, has_side_effects=True, vmem_limit_bytes=48 * 1024 * 1024
        ),
        cost_estimate=pl.CostEstimate(
            flops=1_600_000_000, bytes_accessed=20_000_000, transcendentals=0
        ),
        name="ffn",
    )(feat, mixed, w)


def solution(mesh):
    nz, ny = split_sp(mesh)
    sp_tp = P("sp", "tp")
    return jax.shard_map(
        functools.partial(local, nz, ny, mesh.shape["tp"]),
        mesh=mesh,
        in_specs=(P(("sp", "tp"), None),)
        + (sp_tp,) * 8
        + (P("tp", None), P("tp", None), P(), sp_tp, P("tp", "sp")),
        out_specs=P(("sp", "tp"), None),
        check_vma=False,
    )
```

```python
import functools

import jax
import jax.numpy as jnp
from jax import lax
from jax.experimental import pallas as pl
from jax.experimental.pallas import tpu as pltpu
from jax.sharding import PartitionSpec as P

A_DIM = 32
B_DIM = 64
LOG2E = 1.4426950408889634
FAR = 1e30
MESH = pl.DeviceIdType.MESH
BF = jnp.bfloat16
F32 = jnp.float32


def split_sp(mesh):
    size = mesh.shape["sp"]
    ny = 1
    while ny * ny < size:
        ny *= 2
    return size // ny, ny


def rcopy(src, dst, send, recv, device):
    return pltpu.make_async_remote_copy(
        src_ref=src,
        dst_ref=dst,
        send_sem=send,
        recv_sem=recv,
        device_id=device,
        device_id_type=MESH,
    )


def nt_dot(a, b):
    return lax.dot_general(a, b, (((1,), (1,)), ((), ())), preferred_element_type=F32)


def head_mask(shape):
    lane = lax.broadcasted_iota(jnp.int32, shape, 1)
    return (lane < A_DIM, (lane >= A_DIM) & (lane < 2 * A_DIM), lane >= 2 * A_DIM)


SCALES = (A_DIM**-0.5 * LOG2E, A_DIM**-0.5 * LOG2E, B_DIM**-0.5 * LOG2E)


class Tp:
    def __init__(self, nx, buf, xs, xr, ds, dr):
        self.nx, self.buf, self.xs, self.xr, self.ds, self.dr = nx, buf, xs, xr, ds, dr
        self.sp, self.tp = lax.axis_index("sp"), lax.axis_index("tp")
        self.x, self.c = self.tp // 2, self.tp % 2

    def across(self, i):
        to = ((self.x + i) % self.nx) * 2 + self.c
        return rcopy(
            self.buf.at[self.tp], self.buf.at[self.tp], self.xs.at[i - 1], self.xr.at[i - 1], (self.sp, to)
        )

    def arrived(self, i):
        return ((self.x - i + self.nx) % self.nx) * 2 + self.c

    def beside(self, i):
        src = self.arrived(i)
        return rcopy(
            self.buf.at[src], self.buf.at[src], self.ds.at[i], self.dr.at[i], (self.sp, self.x * 2 + 1 - self.c)
        )

    def start(self):
        for i in range(1, self.nx):
            self.across(i).start()
        self.beside(0).start()

    def forward(self, i):
        self.across(i).wait_recv()
        self.beside(i).start()

    def finish(self):
        for i in range(self.nx):
            self.beside(i).wait_recv()
        for i in range(1, self.nx):
            self.across(i).wait_send()
        for i in range(self.nx):
            self.beside(i).wait_send()


class Weights:
    def __init__(self, nz, ny, up, down, s1, r1, s2, r2):
        self.nz, self.ny = nz, ny
        self.bufs = (up, down)
        self.s1, self.r1, self.s2, self.r2 = s1, r1, s2, r2
        self.sp, self.tp = lax.axis_index("sp"), lax.axis_index("tp")
        self.z, self.y = self.sp // ny, self.sp % ny

    def shifted(self, along_y, by):
        if along_y:
            return self.z, (self.y + by + self.ny) % self.ny
        return (self.z + by + self.nz) % self.nz, self.y

    def length(self, along_y):
        return self.ny if along_y else self.nz

    def copy(self, phase, half, way, s, chunk, by):
        along_y = (half == 0) == (phase == 1)
        sign = 1 - 2 * way
        z, y = self.shifted(along_y, by)
        buf = self.bufs[half]
        if phase == 1:
            ref = buf.at[z, y]
            if s == self.length(along_y) // 2:
                rows = buf.shape[2] // 2
                ref = buf.at[z, y, way * rows : (way + 1) * rows]
            send, recv = self.s1.at[half, way, s - 1], self.r1.at[half, way, s - 1]
        else:
            if along_y:
                part = self.nz // 2
                ref = buf.at[chunk * part : (chunk + 1) * part, y]
            else:
                part = self.ny // 2
                ref = buf.at[z, chunk * part : (chunk + 1) * part]
            send, recv = self.s2.at[half, way, s - 1, chunk], self.r2.at[half, way, s - 1, chunk]
        tz, ty = self.shifted(along_y, sign)
        return rcopy(ref, ref, send, recv, (tz * self.ny + ty, self.tp))

    def sent(self, phase, half, way, s, chunk=0):
        return self.copy(phase, half, way, s, chunk, -(1 - 2 * way) * (s - 1))

    def landed(self, phase, half, way, s, chunk=0):
        return self.copy(phase, half, way, s, chunk, -(1 - 2 * way) * s)

    def last(self, phase, half):
        return self.length((half == 0) == (phase == 1)) // 2

    def streams(self):
        return [(half, way) for half in (0, 1) for way in (0, 1)]

    def chunks(self, half, way, s):
        return (way,) if s == self.last(2, half) else (0, 1)

    def start(self):
        for half, way in self.streams():
            self.sent(1, half, way, 1).start()

    def step(self, s):
        for half, way in self.streams():
            if s <= self.last(1, half):
                self.landed(1, half, way, s).wait_recv()
                if s < self.last(1, half):
                    self.sent(1, half, way, s + 1).start()

    def lines(self):
        for chunk in (0, 1):
            for half, way in self.streams():
                if chunk in self.chunks(half, way, 1):
                    self.sent(2, half, way, 1, chunk).start()

    def tick(self, k):
        s, chunk = k // 2 + 1, k % 2
        for half, way in self.streams():
            if s <= self.last(2, half) and chunk in self.chunks(half, way, s):
                self.landed(2, half, way, s, chunk).wait_recv()
                if s < self.last(2, half) and chunk in self.chunks(half, way, s + 1):
                    self.sent(2, half, way, s + 1, chunk).start()

    def ticks(self):
        return 2 * max(self.last(2, 0), self.last(2, 1))

    def finish(self):
        for half, way in self.streams():
            for s in range(1, self.last(1, half) + 1):
                self.sent(1, half, way, s).wait_send()
            for s in range(1, self.last(2, half) + 1):
                for chunk in self.chunks(half, way, s):
                    self.sent(2, half, way, s, chunk).wait_send()


def layer(
    nz,
    ny,
    nt,
    qn,
    qb,
    kn,
    kb,
    vn,
    vb,
    gn,
    gb,
    pn,
    pb,
    res_in,
    gain_in,
    up_in,
    down_in,
    out,
    raw,
    graw_n,
    graw_b,
    res,
    gain,
    up,
    down,
    qbuf,
    kbuf,
    vbuf,
    gbuf,
    gk,
    pw,
    osend,
    lsend,
    orecv,
    lrecv,
    asend,
    arecv,
    feat,
    part,
    psum,
    pair,
    got,
    in_sem,
    q_s,
    q_r,
    kv_s,
    kv_r,
    pw_xs,
    pw_xr,
    pw_ds,
    pw_dr,
    p_s,
    p_r,
    a_s,
    a_r,
    f_xs,
    f_xr,
    f_ds,
    f_dr,
    w_s1,
    w_r1,
    w_s2,
    w_r2,
    pair_s,
    pair_r,
    g_s,
    g_r,
):
    nx = nt // 2
    sp, tp = lax.axis_index("sp"), lax.axis_index("tp")
    z, y = sp // ny, sp % ny
    x, core = tp // 2, tp % 2
    tok = qn.shape[1]
    rows, d = res.shape
    keys = nz * tok

    barrier = pltpu.get_barrier_semaphore()
    peers = [(z * ny + (y + i) % ny, tp) for i in range(1, ny)]
    up_z, down_z = ((z + 1) % nz) * ny + y, ((z + nz - 1) % nz) * ny + y
    peers += [(up_z, tp), (down_z, tp)]
    peers += [(sp, (tp + i) % nt) for i in range(1, nt)]
    for peer in peers:
        pl.semaphore_signal(barrier, inc=1, device_id=peer, device_id_type=MESH)

    def load(i, src, dst):
        return pltpu.make_async_copy(src, dst, in_sem.at[i])

    loads = [load(i, r, raw.at[i]) for i, r in enumerate((qn, qb, kn, kb, vn, vb))]
    loads += [load(6, gn, graw_n), load(7, gb, graw_b)]
    load_w = [load(8, up_in, up.at[z, y]), load(9, down_in, down.at[z, y])]
    load_p = [load(10, pn, pw.at[tp, 0:64]), load(11, pb, pw.at[tp, 64:128])]
    load_r = [load(12, res_in, res), load(13, gain_in, gain)]
    for c in loads + load_w + load_p + load_r:
        c.start()

    for r in range(nz):
        vbuf[r, :, 128:256] = jnp.ones((tok, 128), BF)
    for c in loads:
        c.wait()

    qbuf[y, 0:tok, :] = jnp.transpose(raw[0:2].reshape(128, tok))
    kbuf[0] = jnp.transpose(raw[2:4].reshape(128, tok))
    vbuf[0, :, 0:128] = jnp.transpose(raw[4:6].reshape(128, tok))
    lane = lax.broadcasted_iota(jnp.int32, (tok, 128), 1)
    first_lane = lax.broadcasted_iota(jnp.int32, (16, 128), 1)
    starts = jnp.where(
        first_lane == 0,
        graw_n[0:1, 0:1],
        jnp.where(first_lane == 1, graw_n[1:2, 0:1], jnp.where(first_lane == 2, graw_b[0:1, 0:1], 0.0)),
    )
    qbuf[y, tok : tok + 16, :] = starts.astype(BF)
    gbuf[0] = jnp.zeros((8, 256), F32)
    gbuf[0, 0:2, 0:tok] = graw_n[...]
    gbuf[0, 2:3, 0:tok] = graw_b[...]

    for c in load_w + load_p:
        c.wait()
    pl.semaphore_wait(barrier, len(peers))

    weights = Weights(nz, ny, up, down, w_s1, w_r1, w_s2, w_r2)

    def ring(slot, src, to):
        return [
            rcopy(kbuf.at[src], kbuf.at[slot], kv_s.at[0, slot - 1], kv_r.at[0, slot - 1], (to, tp)),
            rcopy(
                vbuf.at[src, :, 0:128],
                vbuf.at[slot, :, 0:128],
                kv_s.at[1, slot - 1],
                kv_r.at[1, slot - 1],
                (to, tp),
            ),
            rcopy(gbuf.at[src], gbuf.at[slot], kv_s.at[2, slot - 1], kv_r.at[2, slot - 1], (to, tp)),
        ]

    rights = nz // 2
    lefts = nz - 1 - rights
    steps = [ring(s, s - 1, up_z) for s in range(1, rights + 1)]
    steps_left = [ring(nz - s, (nz - s + 1) % nz, down_z) for s in range(1, lefts + 1)]

    q_sends = [
        rcopy(
            qbuf.at[y], qbuf.at[y], q_s.at[i - 1], q_r.at[i - 1], (z * ny + (y + i) % ny, tp)
        )
        for i in range(1, ny)
    ]
    for chain in steps[0:1] + steps_left[0:1]:
        for c in chain:
            c.start()
    for c in q_sends:
        c.start()
    weights.start()
    share = Tp(nx, pw, pw_xs, pw_xr, pw_ds, pw_dr)
    share.start()

    for s in range(1, max(rights, weights.last(1, 0), weights.last(1, 1)) + 1):
        if s <= rights:
            for c in steps[s - 1]:
                c.wait_recv()
            if s < rights:
                for c in steps[s]:
                    c.start()
        if s <= lefts:
            for c in steps_left[s - 1]:
                c.wait_recv()
            if s < lefts:
                for c in steps_left[s]:
                    c.start()
        weights.step(s)
    weights.lines()

    for r in range(nz):
        gk[:, r * tok : (r + 1) * tok] = jnp.where(r <= z, gbuf[r, :, 0:tok], FAR)

    col = lax.broadcasted_iota(jnp.int32, (1, keys), 1)

    def block(src, own, out_o, out_l):
        q = qbuf[src, 0:tok, :]
        masks = head_mask((tok, 128))
        k = kbuf[...].reshape(keys, 128)
        v = vbuf[...].reshape(keys, 256)
        outs, lses = [], []
        for h in range(3):
            s = nt_dot(jnp.where(masks[h], q, jnp.zeros_like(q)), k)
            ref = qbuf[src, tok : tok + 16, :][0:1, h : h + 1].astype(F32)
            bias = (ref - gk[h : h + 1, :]) * LOG2E
            if not own:
                bias = jnp.where((col < tok) & (y > src), -FAR, bias)
            s = s * SCALES[h] + bias
            if own:
                wide = min(keys, 256)
                first = s[:, 0:wide]
                at = lax.broadcasted_iota(jnp.int32, first.shape, 1)
                row = lax.broadcasted_iota(jnp.int32, first.shape, 0)
                first = jnp.where((at < tok) & (at > row), -FAR, first)
                s = jnp.concatenate([first, s[:, wide:]], axis=1) if keys > wide else first
            m = jnp.max(s, axis=1, keepdims=True)
            w = jnp.exp2(s - m).astype(BF)
            o = jnp.dot(w, v, preferred_element_type=F32)
            total = o[:, 128:256]
            outs.append(o[:, 0:128] / total)
            lses.append(m + jnp.log2(total))
        out_o[...] = jnp.where(masks[0], outs[0], jnp.where(masks[1], outs[1], outs[2])).astype(BF)
        lse = jnp.where(lane == 0, lses[0], jnp.where(lane == 1, lses[1], lses[2]))
        out_l[:, 0:tok] = jnp.transpose(lse)[0:8]

    def give(i):
        src = (y + ny - i) % ny
        to = (z * ny + src, tp)
        return [
            rcopy(osend.at[i - 1], orecv.at[y], p_s.at[0, i - 1], p_r.at[0, i - 1], to),
            rcopy(lsend.at[i - 1], lrecv.at[y], p_s.at[1, i - 1], p_r.at[1, i - 1], to),
        ]

    def one(i, carry):
        src = (y + ny - i) % ny
        rcopy(qbuf.at[y], qbuf.at[src], q_s.at[i - 1], q_r.at[i - 1], (z * ny + src, tp)).wait_recv()
        block(src, False, osend.at[i - 1], lsend.at[i - 1])
        for c in give(i):
            c.start()
        return carry

    tick = 0
    ticks = weights.ticks()
    cuts = [1, 4, 7, 8] if ny == 8 else [1, ny]
    for a, b in zip(cuts[:-1], cuts[1:]):
        lax.fori_loop(a, b, one, 0)
        if tick < ticks:
            weights.tick(tick)
            tick += 1
    block(y, True, orecv.at[y], lrecv.at[y])
    for i in range(1, nx):
        share.forward(i)
    if tick < ticks:
        weights.tick(tick)
        tick += 1
    for i in range(1, ny):
        for c in give(i):
            c.wait_recv()

    lse = [lrecv[j, :, 0:tok] for j in range(ny)]
    peak = functools.reduce(jnp.maximum, lse)
    parts = [jnp.exp2(a - peak) for a in lse]
    inv = 1.0 / functools.reduce(jnp.add, parts)
    share_t = jnp.transpose(jnp.concatenate([a * inv for a in parts], axis=0))
    masks = head_mask((tok, 128))
    att = jnp.zeros((tok, 128), F32)
    for j in range(ny):
        f = [share_t[:, 8 * j + h : 8 * j + h + 1] for h in range(3)]
        factor = jnp.where(masks[0], f[0], jnp.where(masks[1], f[1], f[2]))
        att = att + factor * orecv[j].astype(F32)
    for t in range(nt):
        asend[t] = att[t * rows : (t + 1) * rows].astype(BF)

    def hand(i):
        to = (tp + i) % nt
        return rcopy(asend.at[to], arecv.at[tp], a_s.at[i - 1], a_r.at[i - 1], (sp, to))

    for i in range(1, nt):
        hand(i).start()
    arecv[tp] = asend[tp]
    share.finish()
    if tick < ticks:
        weights.tick(tick)
        tick += 1
    for i in range(1, nt):
        hand(i).wait_recv()

    full = jnp.concatenate([arecv[t] for t in range(nt)], axis=1)
    projected = jnp.dot(full, pw[...].reshape(nt * 128, d), preferred_element_type=F32)
    for c in load_r:
        c.wait()
    mixed = (res[...].astype(F32) + projected).astype(BF)
    wide = mixed.astype(F32)
    scale = lax.rsqrt(jnp.mean(wide * wide, axis=-1, keepdims=True) + 1e-6)
    feat[tp] = (wide * scale * gain[...]).astype(BF)

    spread = Tp(nx, feat, f_xs, f_xr, f_ds, f_dr)
    spread.start()
    if tick < ticks:
        weights.tick(tick)
        tick += 1
    for i in range(1, nx):
        spread.forward(i)
    while tick < ticks:
        weights.tick(tick)
        tick += 1
    spread.finish()

    ff = up.shape[3]
    h = jnp.dot(feat[...].reshape(nt * rows, d), up[...].reshape(d, ff), preferred_element_type=F32)
    h = jnp.square(jnp.maximum(h, 0.0)).astype(BF)
    total = nt_dot(h, down[...].reshape(d, ff))
    for t in range(nt):
        piece = total[t * rows : (t + 1) * rows]

        @pl.when(core == t % 2)
        def _():
            part[t // 2] = piece

        @pl.when(core != t % 2)
        def _():
            psum[t // 2] = piece.astype(BF)

    beside = (sp, x * 2 + 1 - core)
    swap = rcopy(psum, pair, pair_s, pair_r, beside)
    swap.start()
    swap.wait()

    def spare(i):
        to = (x + i) % nx
        return rcopy(psum.at[to], got.at[i - 1], g_s.at[i - 1], g_r.at[i - 1], (sp, to * 2 + core))

    for i in range(1, nx):
        to = (x + i) % nx
        psum[to] = (part[to] + pair[to].astype(F32)).astype(BF)
        spare(i).start()
    acc = wide + (part[x] + pair[x].astype(F32))
    for i in range(1, nx):
        spare(i).wait_recv()
        acc = acc + got[i - 1].astype(F32)
    out[...] = acc.astype(BF)

    for i in range(1, nx):
        spare(i).wait_send()
    weights.finish()
    for chain in steps + steps_left:
        for c in chain:
            c.wait_send()
    for c in q_sends:
        c.wait_send()
    for i in range(1, ny):
        for c in give(i):
            c.wait_send()
    for i in range(1, nt):
        hand(i).wait_send()


def local(nz, ny, nt, *args):
    res, qn, kn, vn, qb, kb, vb, gn, gb, pn, pb, gain, up, down = args
    tok = qn.shape[0]
    rows, d = res.shape
    nx = nt // 2
    band, ff = up.shape

    dma = pltpu.SemaphoreType.DMA
    anyw = pl.BlockSpec(memory_space=pl.ANY)
    return pl.pallas_call(
        functools.partial(layer, nz, ny, nt),
        out_shape=jax.ShapeDtypeStruct((rows, d), BF),
        in_specs=[anyw] * 14,
        out_specs=pl.BlockSpec(memory_space=pltpu.VMEM),
        scratch_shapes=[
            pltpu.VMEM((6, 64, tok), BF),
            pltpu.VMEM((2, tok), F32),
            pltpu.VMEM((1, tok), F32),
            pltpu.VMEM((rows, d), BF),
            pltpu.VMEM((1, d), F32),
            pltpu.VMEM((nz, ny, band, ff), BF),
            pltpu.VMEM((nz, ny, band, ff), BF),
            pltpu.VMEM((ny, tok + 16, 128), BF),
            pltpu.VMEM((nz, tok, 128), BF),
            pltpu.VMEM((nz, tok, 256), BF),
            pltpu.VMEM((nz, 8, 256), F32),
            pltpu.VMEM((8, nz * tok), F32),
            pltpu.VMEM((nt, 128, d), BF),
            pltpu.VMEM((ny - 1, tok, 128), BF),
            pltpu.VMEM((ny - 1, 8, 256), F32),
            pltpu.VMEM((ny, tok, 128), BF),
            pltpu.VMEM((ny, 8, 256), F32),
            pltpu.VMEM((nt, rows, 128), BF),
            pltpu.VMEM((nt, rows, 128), BF),
            pltpu.VMEM((nt, rows, d), BF),
            pltpu.VMEM((nx, rows, d), F32),
            pltpu.VMEM((nx, rows, d), BF),
            pltpu.VMEM((nx, rows, d), BF),
            pltpu.VMEM((nx - 1, rows, d), BF),
            dma((14,)),
            dma((ny - 1,)),
            dma((ny - 1,)),
            dma((3, nz - 1)),
            dma((3, nz - 1)),
            dma((nx - 1,)),
            dma((nx - 1,)),
            dma((nx,)),
            dma((nx,)),
            dma((2, ny - 1)),
            dma((2, ny - 1)),
            dma((nt - 1,)),
            dma((nt - 1,)),
            dma((nx - 1,)),
            dma((nx - 1,)),
            dma((nx,)),
            dma((nx,)),
            dma((2, 2, max(ny, nz) // 2)),
            dma((2, 2, max(ny, nz) // 2)),
            dma((2, 2, max(ny, nz) // 2, 2)),
            dma((2, 2, max(ny, nz) // 2, 2)),
            dma,
            dma,
            dma((nx - 1,)),
            dma((nx - 1,)),
        ],
        compiler_params=pltpu.CompilerParams(
            collective_id=0, has_side_effects=True, vmem_limit_bytes=64 * 1024 * 1024 - 65536
        ),
        name="layer",
    )(qn.T, qb.T, kn.T, kb.T, vn.T, vb.T, gn.T, gb.T, pn, pb, res, gain.reshape(1, d), up, down.T)


def solution(mesh):
    nz, ny = split_sp(mesh)
    sp_tp = P("sp", "tp")
    return jax.shard_map(
        functools.partial(local, nz, ny, mesh.shape["tp"]),
        mesh=mesh,
        in_specs=(P(("sp", "tp"), None),)
        + (sp_tp,) * 8
        + (P("tp", None), P("tp", None), P(), sp_tp, P("tp", "sp")),
        out_specs=P(("sp", "tp"), None),
        check_vma=False,
    )
```

```python
import functools

import jax
import jax.numpy as jnp
from jax import lax
from jax.experimental import pallas as pl
from jax.experimental.pallas import tpu as pltpu
from jax.sharding import PartitionSpec as P

A_DIM = 32
B_DIM = 64
LOG2E = 1.4426950408889634
FAR = 1e30
MESH = pl.DeviceIdType.MESH
BF = jnp.bfloat16
F32 = jnp.float32


def split_sp(mesh):
    size = mesh.shape["sp"]
    ny = 1
    while ny * ny < size:
        ny *= 2
    return size // ny, ny


def rcopy(src, dst, send, recv, device):
    return pltpu.make_async_remote_copy(
        src_ref=src,
        dst_ref=dst,
        send_sem=send,
        recv_sem=recv,
        device_id=device,
        device_id_type=MESH,
    )


def nt_dot(a, b):
    return lax.dot_general(a, b, (((1,), (1,)), ((), ())), preferred_element_type=F32)


def head_mask(shape):
    lane = lax.broadcasted_iota(jnp.int32, shape, 1)
    return (lane < A_DIM, (lane >= A_DIM) & (lane < 2 * A_DIM), lane >= 2 * A_DIM)


SCALES = (A_DIM**-0.5 * LOG2E, A_DIM**-0.5 * LOG2E, B_DIM**-0.5 * LOG2E)


class Tp:
    def __init__(self, nx, buf, xs, xr, ds, dr):
        self.nx, self.buf, self.xs, self.xr, self.ds, self.dr = nx, buf, xs, xr, ds, dr
        self.sp, self.tp = lax.axis_index("sp"), lax.axis_index("tp")
        self.x, self.c = self.tp // 2, self.tp % 2

    def across(self, i):
        to = ((self.x + i) % self.nx) * 2 + self.c
        return rcopy(
            self.buf.at[self.tp], self.buf.at[self.tp], self.xs.at[i - 1], self.xr.at[i - 1], (self.sp, to)
        )

    def arrived(self, i):
        return ((self.x - i + self.nx) % self.nx) * 2 + self.c

    def beside(self, i):
        src = self.arrived(i)
        return rcopy(
            self.buf.at[src], self.buf.at[src], self.ds.at[i], self.dr.at[i], (self.sp, self.x * 2 + 1 - self.c)
        )

    def start(self):
        for i in range(1, self.nx):
            self.across(i).start()
        self.beside(0).start()

    def forward(self, i):
        self.across(i).wait_recv()
        self.beside(i).start()

    def finish(self):
        for i in range(self.nx):
            self.beside(i).wait_recv()
        for i in range(1, self.nx):
            self.across(i).wait_send()
        for i in range(self.nx):
            self.beside(i).wait_send()


class Weights:
    def __init__(self, nz, ny, src, buf, d_s, d_r, w_s, w_r):
        self.nz, self.ny, self.src, self.buf = nz, ny, src, buf
        self.d_s, self.d_r, self.w_s, self.w_r = d_s, d_r, w_s, w_r
        self.sp, self.tp = lax.axis_index("sp"), lax.axis_index("tp")
        self.z, self.y = self.sp // ny, self.sp % ny
        self.x, self.core = self.tp // 2, self.tp % 2
        self.width = buf.shape[4]
        self.mine = self.y % 2 == self.core
        self.last = nz // 2

    def half(self, c):
        return pl.ds(pl.multiple_of(c * self.width, self.width), self.width)

    def deal(self, t, c):
        to_y = ((self.y // 2 + t) % (self.ny // 2)) * 2 + self.core
        return rcopy(
            self.src.at[:, :, self.half(c)],
            self.buf.at[self.z, self.y],
            self.d_s.at[t, c],
            self.d_r.at[self.y],
            (self.z * self.ny + to_y, self.x * 2 + c),
        )

    def start(self):
        @pl.when(self.mine)
        def _():
            self.buf[self.z, self.y] = self.src[:, :, self.half(self.core)]

        @pl.when(jnp.logical_not(self.mine))
        def _():
            self.deal(0, self.core).start()

        self.deal(0, 1 - self.core).start()
        n = self.ny // 2
        for t in sorted(range(1, n), key=lambda t: min(t, n - t)):
            for c in (0, 1):
                self.deal(t, c).start()

    def place(self, k):
        far = (k + 1) // 2
        return (self.y + far * (2 * (k % 2) - 1) + self.ny) % self.ny

    def copy(self, way, s, k, by):
        sign = 1 - 2 * way
        ref = self.buf.at[(self.z - sign * by + self.nz) % self.nz, self.place(k)]
        to = (self.z + sign + self.nz) % self.nz
        return rcopy(
            ref, ref, self.w_s.at[way, s - 1, k], self.w_r.at[way, s - 1, k], (to * self.ny + self.y, self.tp)
        )

    def ways(self, s, k):
        return (k % 2,) if s == self.last else (0, 1)

    def own(self, k):
        def arrived():
            at = self.place(k)
            rcopy(
                self.src.at[:, :, self.half(self.core)],
                self.buf.at[self.z, at],
                self.d_s.at[0, 0],
                self.d_r.at[at],
                (self.sp, self.x * 2 + 1 - self.core),
            ).wait_recv()

        if k == 0:
            pl.when(jnp.logical_not(self.mine))(arrived)
        else:
            arrived()
        for way in self.ways(1, k):
            self.copy(way, 1, k, 0).start()

    def tick(self, t):
        s, k = t // self.ny + 1, t % self.ny
        for way in self.ways(s, k):
            self.copy(way, s, k, s).wait_recv()
        if s < self.last:
            for way in self.ways(s + 1, k):
                self.copy(way, s + 1, k, s).start()

    def tick_inner(self, t):
        s, k = t // self.ny + 1, t % self.ny
        for way in (0, 1):
            self.copy(way, s, k, s).wait_recv()

            @pl.when((s + 1 < self.last) | (k % 2 == way))
            def _():
                self.copy(way, s + 1, k, s).start()

    def ticks(self):
        return self.last * self.ny

    def finish(self):
        @pl.when(jnp.logical_not(self.mine))
        def _():
            self.deal(0, self.core).wait_send()

        self.deal(0, 1 - self.core).wait_send()
        for t in range(1, self.ny // 2):
            for c in (0, 1):
                self.deal(t, c).wait_send()
        for s in range(1, self.last + 1):
            for k in range(self.ny):
                for way in self.ways(s, k):
                    self.copy(way, s, k, s - 1).wait_send()


def layer(
    nz,
    ny,
    nt,
    qn,
    qb,
    kn,
    kb,
    vn,
    vb,
    gn,
    gb,
    pn,
    pb,
    res_in,
    gain_in,
    up_in,
    down_in,
    out,
    raw,
    graw_n,
    graw_b,
    res,
    gain,
    wsrc,
    wbuf,
    qbuf,
    kbuf,
    vbuf,
    gbuf,
    gk,
    pw,
    osend,
    lsend,
    orecv,
    lrecv,
    asend,
    arecv,
    feat,
    part,
    psum,
    pair,
    xsend,
    got,
    ysend,
    yrecv,
    in_sem,
    q_s,
    q_r,
    kv_s,
    kv_r,
    pw_xs,
    pw_xr,
    pw_ds,
    pw_dr,
    p_s,
    p_r,
    a_s,
    a_r,
    f_s,
    f_r,
    f_xs,
    f_xr,
    f_ds,
    f_dr,
    d_s,
    d_r,
    w_s,
    w_r,
    pair_s,
    pair_r,
    g_s,
    g_r,
    y_s,
    y_r,
):
    nx = nt // 2
    sp, tp = lax.axis_index("sp"), lax.axis_index("tp")
    z, y = sp // ny, sp % ny
    x, core = tp // 2, tp % 2
    tok = qn.shape[1]
    rows, d = res.shape
    keys = nz * tok

    barrier = pltpu.get_barrier_semaphore()
    peers = [(z * ny + (y + i) % ny, tp) for i in range(1, ny)]
    up_z, down_z = ((z + 1) % nz) * ny + y, ((z + nz - 1) % nz) * ny + y
    other = x * 2 + 1 - core
    peers += [(z * ny + (y + i) % ny, other) for i in range(1, ny)]
    peers += [(up_z, tp), (down_z, tp)]
    peers += [(sp, (tp + i) % nt) for i in range(1, nt)]
    for peer in peers:
        pl.semaphore_signal(barrier, inc=1, device_id=peer, device_id_type=MESH)

    def load(i, src, dst):
        return pltpu.make_async_copy(src, dst, in_sem.at[i])

    loads = [load(i, r, raw.at[i]) for i, r in enumerate((qn, qb, kn, kb, vn, vb))]
    loads += [load(6, gn, graw_n), load(7, gb, graw_b)]
    load_w = [load(8, up_in, wsrc.at[0]), load(9, down_in, wsrc.at[1])]
    load_p = [load(10, pn, pw.at[tp, 0:64]), load(11, pb, pw.at[tp, 64:128])]
    load_r = [load(12, res_in, res), load(13, gain_in, gain)]
    for c in loads + load_w + load_p + load_r:
        c.start()

    for r in range(nz):
        vbuf[r, :, 128:256] = jnp.ones((tok, 128), BF)
    for c in loads:
        c.wait()

    qbuf[y, 0:tok, :] = jnp.transpose(raw[0:2].reshape(128, tok))
    kbuf[0] = jnp.transpose(raw[2:4].reshape(128, tok))
    vbuf[0, :, 0:128] = jnp.transpose(raw[4:6].reshape(128, tok))
    lane = lax.broadcasted_iota(jnp.int32, (tok, 128), 1)
    first_lane = lax.broadcasted_iota(jnp.int32, (16, 128), 1)
    starts = jnp.where(
        first_lane == 0,
        graw_n[0:1, 0:1],
        jnp.where(first_lane == 1, graw_n[1:2, 0:1], jnp.where(first_lane == 2, graw_b[0:1, 0:1], 0.0)),
    )
    qbuf[y, tok : tok + 16, :] = starts.astype(BF)
    gbuf[0] = jnp.zeros((8, 256), F32)
    gbuf[0, 0:2, 0:tok] = graw_n[...]
    gbuf[0, 2:3, 0:tok] = graw_b[...]

    for c in load_w + load_p:
        c.wait()
    pl.semaphore_wait(barrier, len(peers))

    weights = Weights(nz, ny, wsrc, wbuf, d_s, d_r, w_s, w_r)

    def ring(slot, src, to):
        return [
            rcopy(kbuf.at[src], kbuf.at[slot], kv_s.at[0, slot - 1], kv_r.at[0, slot - 1], (to, tp)),
            rcopy(
                vbuf.at[src, :, 0:128],
                vbuf.at[slot, :, 0:128],
                kv_s.at[1, slot - 1],
                kv_r.at[1, slot - 1],
                (to, tp),
            ),
            rcopy(gbuf.at[src], gbuf.at[slot], kv_s.at[2, slot - 1], kv_r.at[2, slot - 1], (to, tp)),
        ]

    rights = nz // 2
    lefts = nz - 1 - rights
    steps = [ring(s, s - 1, up_z) for s in range(1, rights + 1)]
    steps_left = [ring(nz - s, (nz - s + 1) % nz, down_z) for s in range(1, lefts + 1)]

    def q_ring(way, s, by):
        sign = 1 - 2 * way
        ref = qbuf.at[(y - sign * by + ny) % ny]
        return rcopy(
            ref, ref, q_s.at[way, s - 1], q_r.at[way, s - 1], (z * ny + (y + sign + ny) % ny, tp)
        )

    q_last = (ny // 2, ny - 1 - ny // 2)
    for chain in steps[0:1] + steps_left[0:1]:
        for c in chain:
            c.start()
    for way in (0, 1):
        if q_last[way] > 0:
            q_ring(way, 1, 0).start()
    weights.start()
    share = Tp(nx, pw, pw_xs, pw_xr, pw_ds, pw_dr)
    share.start()

    most = max(rights, q_last[0])
    line = 0
    for s in range(1, most + 1):
        if s <= rights:
            for c in steps[s - 1]:
                c.wait_recv()
            if s < rights:
                for c in steps[s]:
                    c.start()
        if s <= lefts:
            for c in steps_left[s - 1]:
                c.wait_recv()
            if s < lefts:
                for c in steps_left[s]:
                    c.start()
        for way in (0, 1):
            if s <= q_last[way]:
                q_ring(way, s, s).wait_recv()
                if s < q_last[way]:
                    q_ring(way, s + 1, s).start()
        while line < ny * s // most:
            weights.own(line)
            line += 1

    for r in range(nz):
        gk[:, r * tok : (r + 1) * tok] = jnp.where(r <= z, gbuf[r, :, 0:tok], FAR)

    col = lax.broadcasted_iota(jnp.int32, (1, keys), 1)

    def block(src, own, out_o, out_l):
        q = qbuf[src, 0:tok, :]
        masks = head_mask((tok, 128))
        k = kbuf[...].reshape(keys, 128)
        v = vbuf[...].reshape(keys, 256)
        outs, lses = [], []
        for h in range(3):
            s = nt_dot(jnp.where(masks[h], q, jnp.zeros_like(q)), k)
            ref = qbuf[src, tok : tok + 16, :][0:1, h : h + 1].astype(F32)
            bias = (ref - gk[h : h + 1, :]) * LOG2E
            if not own:
                bias = jnp.where((col < tok) & (y > src), -FAR, bias)
            s = s * SCALES[h] + bias
            if own:
                wide = min(keys, 256)
                first = s[:, 0:wide]
                at = lax.broadcasted_iota(jnp.int32, first.shape, 1)
                row = lax.broadcasted_iota(jnp.int32, first.shape, 0)
                first = jnp.where((at < tok) & (at > row), -FAR, first)
                s = jnp.concatenate([first, s[:, wide:]], axis=1) if keys > wide else first
            m = jnp.max(s, axis=1, keepdims=True)
            w = jnp.exp2(s - m).astype(BF)
            o = jnp.dot(w, v, preferred_element_type=F32)
            total = o[:, 128:256]
            outs.append(o[:, 0:128] / total)
            lses.append(m + jnp.log2(total))
        out_o[...] = jnp.where(masks[0], outs[0], jnp.where(masks[1], outs[1], outs[2])).astype(BF)
        lse = jnp.where(lane == 0, lses[0], jnp.where(lane == 1, lses[1], lses[2]))
        out_l[:, 0:tok] = jnp.transpose(lse)[0:8]

    def give(i):
        src = (y + ny - i) % ny
        to = (z * ny + src, tp)
        return [
            rcopy(osend.at[i - 1], orecv.at[y], p_s.at[0, i - 1], p_r.at[0, i - 1], to),
            rcopy(lsend.at[i - 1], lrecv.at[y], p_s.at[1, i - 1], p_r.at[1, i - 1], to),
        ]

    def one(i, carry):
        src = (y + ny - i) % ny
        block(src, False, osend.at[i - 1], lsend.at[i - 1])
        for c in give(i):
            c.start()
        return carry

    ticks = weights.ticks()
    inner = max(0, ticks - ny)
    per = min(2, inner // (ny - 1))

    def paced(i, carry):
        one(i, carry)
        for j in range(per):
            weights.tick_inner((i - 1) * per + j)
        return carry

    lax.fori_loop(1, ny, paced, 0)
    todo = list(range(per * (ny - 1), ticks))

    def go(count):
        for t in todo[:count]:
            weights.tick(t)
        del todo[:count]

    block(y, True, orecv.at[y], lrecv.at[y])
    for i in range(1, nx):
        share.forward(i)
    go(3)
    for i in range(1, ny):
        for c in give(i):
            c.wait_recv()

    lse = [lrecv[j, :, 0:tok] for j in range(ny)]
    peak = functools.reduce(jnp.maximum, lse)
    parts = [jnp.exp2(a - peak) for a in lse]
    inv = 1.0 / functools.reduce(jnp.add, parts)
    share_t = jnp.transpose(jnp.concatenate([a * inv for a in parts], axis=0))
    masks = head_mask((tok, 128))
    att = jnp.zeros((tok, 128), F32)
    for j in range(ny):
        f = [share_t[:, 8 * j + h : 8 * j + h + 1] for h in range(3)]
        factor = jnp.where(masks[0], f[0], jnp.where(masks[1], f[1], f[2]))
        att = att + factor * orecv[j].astype(F32)
    for t in range(nt):
        asend[t] = att[t * rows : (t + 1) * rows].astype(BF)

    def hand(i):
        to = (tp + i) % nt
        return rcopy(asend.at[to], arecv.at[tp], a_s.at[i - 1], a_r.at[i - 1], (sp, to))

    for i in range(1, nt):
        hand(i).start()
    arecv[tp] = asend[tp]
    share.finish()
    go(2)
    for i in range(1, nt):
        hand(i).wait_recv()

    full = jnp.concatenate([arecv[t] for t in range(nt)], axis=1)
    projected = jnp.dot(full, pw[...].reshape(nt * 128, d), preferred_element_type=F32)
    for c in load_r:
        c.wait()
    mixed = (res[...].astype(F32) + projected).astype(BF)
    wide = mixed.astype(F32)
    scale = lax.rsqrt(jnp.mean(wide * wide, axis=-1, keepdims=True) + 1e-6)
    half = y % 2
    feat[half, tp] = (wide * scale * gain[...]).astype(BF)
    partner = (z * ny + y + 1 - 2 * half, tp)
    near = Tp(nx, feat.at[half], f_xs.at[0], f_xr.at[0], f_ds.at[0], f_dr.at[0])
    far = Tp(nx, feat.at[1 - half], f_xs.at[1], f_xr.at[1], f_ds.at[1], f_dr.at[1])

    def across_y(which):
        return rcopy(feat.at[which, tp], feat.at[which, tp], f_s, f_r, partner)

    across_y(half).start()
    near.start()
    go(2)
    across_y(1 - half).wait_recv()
    far.start()
    go(2)
    for i in range(1, nx):
        near.forward(i)
    go(2)
    for i in range(1, nx):
        far.forward(i)
    go(len(todo))
    near.finish()
    far.finish()

    count = 2 * nt * rows
    ff = wbuf.shape[4]
    h = jnp.dot(feat[...].reshape(count, d), wbuf[:, :, 0].reshape(d, ff), preferred_element_type=F32)
    h = jnp.square(jnp.maximum(h, 0.0)).astype(BF)
    total = nt_dot(h, wbuf[:, :, 1].reshape(d, ff))
    for g in range(2):
        for t in range(nt):
            at = (g * nt + t) * rows
            piece = total[at : at + rows]

            @pl.when(core == t % 2)
            def _():
                part[t // 2, g] = piece

            @pl.when(core != t % 2)
            def _():
                psum[t // 2, g] = piece.astype(BF)

    swap = rcopy(psum, pair, pair_s, pair_r, (sp, other))
    swap.start()
    swap.wait()

    def spare(i):
        to = (x + i) % nx
        return rcopy(xsend.at[i - 1], got.at[i - 1], g_s.at[i - 1], g_r.at[i - 1], (sp, to * 2 + core))

    for i in range(1, nx):
        to = (x + i) % nx
        xsend[i - 1] = (part[to] + pair[to].astype(F32)).astype(BF)
        spare(i).start()
    for i in range(1, nx):
        spare(i).wait_recv()

    def gathered(g):
        acc = part[x, g] + pair[x, g].astype(F32)
        for i in range(1, nx):
            acc = acc + got[i - 1, g].astype(F32)
        return acc

    ysend[...] = gathered(1 - half).astype(BF)
    back = rcopy(ysend, yrecv, y_s, y_r, partner)
    back.start()
    acc = wide + gathered(half)
    back.wait_recv()
    out[...] = (acc + yrecv[...].astype(F32)).astype(BF)

    back.wait_send()
    across_y(half).wait_send()
    for i in range(1, nx):
        spare(i).wait_send()
    weights.finish()
    for chain in steps + steps_left:
        for c in chain:
            c.wait_send()
    for way in (0, 1):
        for s in range(1, q_last[way] + 1):
            q_ring(way, s, s - 1).wait_send()
    for i in range(1, ny):
        for c in give(i):
            c.wait_send()
    for i in range(1, nt):
        hand(i).wait_send()


def local(nz, ny, nt, *args):
    res, qn, kn, vn, qb, kb, vb, gn, gb, pn, pb, gain, up, down = args
    tok = qn.shape[0]
    rows, d = res.shape
    nx = nt // 2
    band, ff = up.shape

    dma = pltpu.SemaphoreType.DMA
    anyw = pl.BlockSpec(memory_space=pl.ANY)
    return pl.pallas_call(
        functools.partial(layer, nz, ny, nt),
        out_shape=jax.ShapeDtypeStruct((rows, d), BF),
        in_specs=[anyw] * 14,
        out_specs=pl.BlockSpec(memory_space=pltpu.VMEM),
        scratch_shapes=[
            pltpu.VMEM((6, 64, tok), BF),
            pltpu.VMEM((2, tok), F32),
            pltpu.VMEM((1, tok), F32),
            pltpu.VMEM((rows, d), BF),
            pltpu.VMEM((1, d), F32),
            pltpu.VMEM((2, band, ff), BF),
            pltpu.VMEM((nz, ny, 2, band, ff // 2), BF),
            pltpu.VMEM((ny, tok + 16, 128), BF),
            pltpu.VMEM((nz, tok, 128), BF),
            pltpu.VMEM((nz, tok, 256), BF),
            pltpu.VMEM((nz, 8, 256), F32),
            pltpu.VMEM((8, nz * tok), F32),
            pltpu.VMEM((nt, 128, d), BF),
            pltpu.VMEM((ny - 1, tok, 128), BF),
            pltpu.VMEM((ny - 1, 8, 256), F32),
            pltpu.VMEM((ny, tok, 128), BF),
            pltpu.VMEM((ny, 8, 256), F32),
            pltpu.VMEM((nt, rows, 128), BF),
            pltpu.VMEM((nt, rows, 128), BF),
            pltpu.VMEM((2, nt, rows, d), BF),
            pltpu.VMEM((nx, 2, rows, d), F32),
            pltpu.VMEM((nx, 2, rows, d), BF),
            pltpu.VMEM((nx, 2, rows, d), BF),
            pltpu.VMEM((nx - 1, 2, rows, d), BF),
            pltpu.VMEM((nx - 1, 2, rows, d), BF),
            pltpu.VMEM((rows, d), BF),
            pltpu.VMEM((rows, d), BF),
            dma((14,)),
            dma((2, ny // 2)),
            dma((2, ny // 2)),
            dma((3, nz - 1)),
            dma((3, nz - 1)),
            dma((nx - 1,)),
            dma((nx - 1,)),
            dma((nx,)),
            dma((nx,)),
            dma((2, ny - 1)),
            dma((2, ny - 1)),
            dma((nt - 1,)),
            dma((nt - 1,)),
            dma,
            dma,
            dma((2, nx - 1)),
            dma((2, nx - 1)),
            dma((2, nx)),
            dma((2, nx)),
            dma((ny // 2, 2)),
            dma((ny,)),
            dma((2, nz // 2, ny)),
            dma((2, nz // 2, ny)),
            dma,
            dma,
            dma((nx - 1,)),
            dma((nx - 1,)),
            dma,
            dma,
        ],
        compiler_params=pltpu.CompilerParams(
            collective_id=0, has_side_effects=True, vmem_limit_bytes=64 * 1024 * 1024 - 65536
        ),
        name="layer",
    )(qn.T, qb.T, kn.T, kb.T, vn.T, vb.T, gn.T, gb.T, pn, pb, res, gain.reshape(1, d), up, down.T)


def solution(mesh):
    nz, ny = split_sp(mesh)
    sp_tp = P("sp", "tp")
    return jax.shard_map(
        functools.partial(local, nz, ny, mesh.shape["tp"]),
        mesh=mesh,
        in_specs=(P(("sp", "tp"), None),)
        + (sp_tp,) * 8
        + (P("tp", None), P("tp", None), P(), sp_tp, P("tp", "sp")),
        out_specs=P(("sp", "tp"), None),
        check_vma=False,
    )
```

```python
import functools

import jax
import jax.numpy as jnp
from jax import lax
from jax.experimental import pallas as pl
from jax.experimental.pallas import tpu as pltpu
from jax.sharding import PartitionSpec as P

A_DIM = 32
B_DIM = 64
LOG2E = 1.4426950408889634
FAR = 1e30
MESH = pl.DeviceIdType.MESH
BF = jnp.bfloat16
F32 = jnp.float32


def split_sp(mesh):
    size = mesh.shape["sp"]
    ny = 1
    while ny * ny < size:
        ny *= 2
    return size // ny, ny


def rcopy(src, dst, send, recv, device):
    return pltpu.make_async_remote_copy(
        src_ref=src,
        dst_ref=dst,
        send_sem=send,
        recv_sem=recv,
        device_id=device,
        device_id_type=MESH,
    )


def nt_dot(a, b):
    return lax.dot_general(a, b, (((1,), (1,)), ((), ())), preferred_element_type=F32)


def head_mask(shape):
    lane = lax.broadcasted_iota(jnp.int32, shape, 1)
    return (lane < A_DIM, (lane >= A_DIM) & (lane < 2 * A_DIM), lane >= 2 * A_DIM)


SCALES = (A_DIM**-0.5 * LOG2E, A_DIM**-0.5 * LOG2E, B_DIM**-0.5 * LOG2E)


class Tp:
    def __init__(self, nx, buf, xs, xr, ds, dr):
        self.nx, self.buf, self.xs, self.xr, self.ds, self.dr = nx, buf, xs, xr, ds, dr
        self.sp, self.tp = lax.axis_index("sp"), lax.axis_index("tp")
        self.x, self.c = self.tp // 2, self.tp % 2

    def across(self, i):
        to = ((self.x + i) % self.nx) * 2 + self.c
        return rcopy(
            self.buf.at[self.tp], self.buf.at[self.tp], self.xs.at[i - 1], self.xr.at[i - 1], (self.sp, to)
        )

    def arrived(self, i):
        return ((self.x - i + self.nx) % self.nx) * 2 + self.c

    def beside(self, i):
        src = self.arrived(i)
        return rcopy(
            self.buf.at[src], self.buf.at[src], self.ds.at[i], self.dr.at[i], (self.sp, self.x * 2 + 1 - self.c)
        )

    def start(self):
        for i in range(1, self.nx):
            self.across(i).start()
        self.beside(0).start()

    def forward(self, i):
        self.across(i).wait_recv()
        self.beside(i).start()

    def finish(self):
        for i in range(self.nx):
            self.beside(i).wait_recv()
        for i in range(1, self.nx):
            self.across(i).wait_send()
        for i in range(self.nx):
            self.beside(i).wait_send()


class Weights:
    def __init__(self, nz, ny, src, buf, d_s, d_r, w_s, w_r):
        self.nz, self.ny, self.src, self.buf = nz, ny, src, buf
        self.d_s, self.d_r, self.w_s, self.w_r = d_s, d_r, w_s, w_r
        self.sp, self.tp = lax.axis_index("sp"), lax.axis_index("tp")
        self.z, self.y = self.sp // ny, self.sp % ny
        self.x, self.core = self.tp // 2, self.tp % 2
        self.width = buf.shape[4]
        self.mine = self.y % 2 == self.core
        self.last = nz // 2

    def half(self, c):
        return pl.ds(pl.multiple_of(c * self.width, self.width), self.width)

    def deal(self, t, c):
        to_y = ((self.y // 2 + t) % (self.ny // 2)) * 2 + self.core
        return rcopy(
            self.src.at[:, :, self.half(c)],
            self.buf.at[self.z, self.y],
            self.d_s.at[t, c],
            self.d_r.at[self.y],
            (self.z * self.ny + to_y, self.x * 2 + c),
        )

    def start(self):
        @pl.when(self.mine)
        def _():
            self.buf[self.z, self.y] = self.src[:, :, self.half(self.core)]

        @pl.when(jnp.logical_not(self.mine))
        def _():
            self.deal(0, self.core).start()

        self.deal(0, 1 - self.core).start()
        n = self.ny // 2
        self.later = sorted(range(1, n), key=lambda t: min(t, n - t))

    def deal_on(self):
        for t in self.later[:1]:
            for c in (0, 1):
                self.deal(t, c).start()
        del self.later[:1]

    def place(self, k):
        far = (k + 1) // 2
        return (self.y + far * (2 * (k % 2) - 1) + self.ny) % self.ny

    def copy(self, way, s, k, by):
        sign = 1 - 2 * way
        ref = self.buf.at[(self.z - sign * by + self.nz) % self.nz, self.place(k)]
        to = (self.z + sign + self.nz) % self.nz
        return rcopy(
            ref, ref, self.w_s.at[way, s - 1, k], self.w_r.at[way, s - 1, k], (to * self.ny + self.y, self.tp)
        )

    def ways(self, s, k):
        return (k % 2,) if s == self.last else (0, 1)

    def own_arrived(self, k):
        at = self.place(k)
        rcopy(
            self.src.at[:, :, self.half(self.core)],
            self.buf.at[self.z, at],
            self.d_s.at[0, 0],
            self.d_r.at[at],
            (self.sp, self.x * 2 + 1 - self.core),
        ).wait_recv()

    def own(self, k):
        if k == 0:
            pl.when(jnp.logical_not(self.mine))(lambda: self.own_arrived(k))
        else:
            self.own_arrived(k)
        for way in self.ways(1, k):
            self.copy(way, 1, k, 0).start()

    def own_inner(self, k):
        self.own_arrived(k)
        for way in (0, 1):

            @pl.when((self.last > 1) | (k % 2 == way))
            def _():
                self.copy(way, 1, k, 0).start()

    def tick(self, t):
        s, k = t // self.ny + 1, t % self.ny
        for way in self.ways(s, k):
            self.copy(way, s, k, s).wait_recv()
        if s < self.last:
            for way in self.ways(s + 1, k):
                self.copy(way, s + 1, k, s).start()

    def tick_inner(self, t):
        s, k = t // self.ny + 1, t % self.ny
        for way in (0, 1):
            self.copy(way, s, k, s).wait_recv()

            @pl.when((s + 1 < self.last) | (k % 2 == way))
            def _():
                self.copy(way, s + 1, k, s).start()

    def ticks(self):
        return self.last * self.ny

    def finish(self):
        @pl.when(jnp.logical_not(self.mine))
        def _():
            self.deal(0, self.core).wait_send()

        self.deal(0, 1 - self.core).wait_send()
        for t in range(1, self.ny // 2):
            for c in (0, 1):
                self.deal(t, c).wait_send()
        for s in range(1, self.last + 1):
            for k in range(self.ny):
                for way in self.ways(s, k):
                    self.copy(way, s, k, s - 1).wait_send()


def layer(
    nz,
    ny,
    nt,
    qn,
    qb,
    kn,
    kb,
    vn,
    vb,
    gn,
    gb,
    pn,
    pb,
    res_in,
    gain_in,
    up_in,
    down_in,
    out,
    raw,
    graw_n,
    graw_b,
    res,
    gain,
    wsrc,
    wbuf,
    qbuf,
    kbuf,
    vbuf,
    gbuf,
    gk,
    pw,
    osend,
    lsend,
    orecv,
    lrecv,
    asend,
    arecv,
    feat,
    hidden,
    part,
    psum,
    pair,
    xsend,
    got,
    ysend,
    yrecv,
    in_sem,
    q_s,
    q_r,
    kv_s,
    kv_r,
    pw_xs,
    pw_xr,
    pw_ds,
    pw_dr,
    p_s,
    p_r,
    a_s,
    a_r,
    f_s,
    f_r,
    f_xs,
    f_xr,
    f_ds,
    f_dr,
    d_s,
    d_r,
    w_s,
    w_r,
    pair_s,
    pair_r,
    g_s,
    g_r,
    y_s,
    y_r,
):
    nx = nt // 2
    sp, tp = lax.axis_index("sp"), lax.axis_index("tp")
    z, y = sp // ny, sp % ny
    x, core = tp // 2, tp % 2
    tok = qn.shape[1]
    rows, d = res.shape
    keys = nz * tok

    barrier = pltpu.get_barrier_semaphore()
    peers = [(z * ny + (y + i) % ny, tp) for i in range(1, ny)]
    up_z, down_z = ((z + 1) % nz) * ny + y, ((z + nz - 1) % nz) * ny + y
    other = x * 2 + 1 - core
    peers += [(z * ny + (y + i) % ny, other) for i in range(1, ny)]
    peers += [(up_z, tp), (down_z, tp)]
    peers += [(sp, (tp + i) % nt) for i in range(1, nt)]
    for peer in peers:
        pl.semaphore_signal(barrier, inc=1, device_id=peer, device_id_type=MESH)

    def load(i, src, dst):
        return pltpu.make_async_copy(src, dst, in_sem.at[i])

    loads = [load(i, r, raw.at[i]) for i, r in enumerate((qn, qb, kn, kb, vn, vb))]
    loads += [load(6, gn, graw_n), load(7, gb, graw_b)]
    load_w = [load(8, up_in, wsrc.at[0]), load(9, down_in, wsrc.at[1])]
    load_p = [load(10, pn, pw.at[tp, 0:64]), load(11, pb, pw.at[tp, 64:128])]
    load_r = [load(12, res_in, res), load(13, gain_in, gain)]
    for c in loads + load_w + load_p + load_r:
        c.start()

    for r in range(nz):
        vbuf[r, :, 128:256] = jnp.ones((tok, 128), BF)
    for c in loads:
        c.wait()

    qbuf[y, 0:tok, :] = jnp.transpose(raw[0:2].reshape(128, tok))
    kbuf[0] = jnp.transpose(raw[2:4].reshape(128, tok))
    vbuf[0, :, 0:128] = jnp.transpose(raw[4:6].reshape(128, tok))
    lane = lax.broadcasted_iota(jnp.int32, (tok, 128), 1)
    first_lane = lax.broadcasted_iota(jnp.int32, (16, 128), 1)
    starts = jnp.where(
        first_lane == 0,
        graw_n[0:1, 0:1],
        jnp.where(first_lane == 1, graw_n[1:2, 0:1], jnp.where(first_lane == 2, graw_b[0:1, 0:1], 0.0)),
    )
    qbuf[y, tok : tok + 16, :] = starts.astype(BF)
    gbuf[0] = jnp.zeros((8, 256), F32)
    gbuf[0, 0:2, 0:tok] = graw_n[...]
    gbuf[0, 2:3, 0:tok] = graw_b[...]

    for c in load_w + load_p:
        c.wait()
    pl.semaphore_wait(barrier, len(peers))

    weights = Weights(nz, ny, wsrc, wbuf, d_s, d_r, w_s, w_r)

    def ring(slot, src, to):
        return [
            rcopy(kbuf.at[src], kbuf.at[slot], kv_s.at[0, slot - 1], kv_r.at[0, slot - 1], (to, tp)),
            rcopy(
                vbuf.at[src, :, 0:128],
                vbuf.at[slot, :, 0:128],
                kv_s.at[1, slot - 1],
                kv_r.at[1, slot - 1],
                (to, tp),
            ),
            rcopy(gbuf.at[src], gbuf.at[slot], kv_s.at[2, slot - 1], kv_r.at[2, slot - 1], (to, tp)),
        ]

    rights = nz // 2
    lefts = nz - 1 - rights
    steps = [ring(s, s - 1, up_z) for s in range(1, rights + 1)]
    steps_left = [ring(nz - s, (nz - s + 1) % nz, down_z) for s in range(1, lefts + 1)]

    def q_ring(way, s, by):
        sign = 1 - 2 * way
        ref = qbuf.at[(y - sign * by + ny) % ny]
        return rcopy(
            ref, ref, q_s.at[way, s - 1], q_r.at[way, s - 1], (z * ny + (y + sign + ny) % ny, tp)
        )

    q_last = (ny // 2, ny - 1 - ny // 2)
    for kind in (2, 0, 1):
        for chain in steps[0:1] + steps_left[0:1]:
            chain[kind].start()
    for way in (0, 1):
        if q_last[way] > 0:
            q_ring(way, 1, 0).start()
    weights.start()
    share = Tp(nx, pw, pw_xs, pw_xr, pw_ds, pw_dr)
    share.start()

    most = max(rights, q_last[0])
    line = 0
    early = min(2, ny)
    for s in range(1, most + 1):
        for kind in (2, 0, 1):
            for chain, end in ((steps, rights), (steps_left, lefts)):
                if s <= end:
                    chain[s - 1][kind].wait_recv()
                    if s < end:
                        chain[s][kind].start()
            if kind == 0:
                for way in (0, 1):
                    if s <= q_last[way]:
                        q_ring(way, s, s).wait_recv()
                        if s < q_last[way]:
                            q_ring(way, s + 1, s).start()
        weights.deal_on()
        if s >= most - 1:
            while line < (early if s == most else early // 2):
                weights.own(line)
                line += 1

    for r in range(nz):
        gk[:, r * tok : (r + 1) * tok] = jnp.where(r <= z, gbuf[r, :, 0:tok], FAR)

    col = lax.broadcasted_iota(jnp.int32, (1, keys), 1)

    def block(src, own, out_o, out_l):
        q = qbuf[src, 0:tok, :]
        masks = head_mask((tok, 128))
        k = kbuf[...].reshape(keys, 128)
        v = vbuf[...].reshape(keys, 256)
        outs, lses = [], []
        for h in range(3):
            s = nt_dot(jnp.where(masks[h], q, jnp.zeros_like(q)), k)
            ref = qbuf[src, tok : tok + 16, :][0:1, h : h + 1].astype(F32)
            bias = (ref - gk[h : h + 1, :]) * LOG2E
            if not own:
                bias = jnp.where((col < tok) & (y > src), -FAR, bias)
            s = s * SCALES[h] + bias
            if own:
                wide = min(keys, 256)
                first = s[:, 0:wide]
                at = lax.broadcasted_iota(jnp.int32, first.shape, 1)
                row = lax.broadcasted_iota(jnp.int32, first.shape, 0)
                first = jnp.where((at < tok) & (at > row), -FAR, first)
                s = jnp.concatenate([first, s[:, wide:]], axis=1) if keys > wide else first
            m = jnp.max(s, axis=1, keepdims=True)
            w = jnp.exp2(s - m).astype(BF)
            o = jnp.dot(w, v, preferred_element_type=F32)
            total = o[:, 128:256]
            outs.append(o[:, 0:128] / total)
            lses.append(m + jnp.log2(total))
        out_o[...] = jnp.where(masks[0], outs[0], jnp.where(masks[1], outs[1], outs[2])).astype(BF)
        lse = jnp.where(lane == 0, lses[0], jnp.where(lane == 1, lses[1], lses[2]))
        out_l[:, 0:tok] = jnp.transpose(lse)[0:8]

    def give(i):
        src = (y + ny - i) % ny
        to = (z * ny + src, tp)
        return [
            rcopy(osend.at[i - 1], orecv.at[y], p_s.at[0, i - 1], p_r.at[0, i - 1], to),
            rcopy(lsend.at[i - 1], lrecv.at[y], p_s.at[1, i - 1], p_r.at[1, i - 1], to),
        ]

    def one(i, carry):
        src = (y + ny - i) % ny
        block(src, False, osend.at[i - 1], lsend.at[i - 1])
        for c in give(i):
            c.start()
        return carry

    ticks = weights.ticks()
    inner = max(0, ticks - ny)
    per = min(1, inner // (ny - 1))

    def paced(i, carry):
        if early < ny:

            @pl.when(i <= ny - early)
            def _():
                weights.own_inner(i + early - 1)

        one(i, carry)
        for j in range(per):
            weights.tick_inner((i - 1) * per + j)
        return carry

    lax.fori_loop(1, ny, paced, 0)
    todo = list(range(per * (ny - 1), ticks))

    def go(count):
        for t in todo[:count]:
            weights.tick(t)
        del todo[:count]

    block(y, True, orecv.at[y], lrecv.at[y])
    for i in range(1, nx):
        share.forward(i)
    go(ny)
    for i in range(1, ny):
        for c in give(i):
            c.wait_recv()

    lse = [lrecv[j, :, 0:tok] for j in range(ny)]
    peak = functools.reduce(jnp.maximum, lse)
    parts = [jnp.exp2(a - peak) for a in lse]
    inv = 1.0 / functools.reduce(jnp.add, parts)
    share_t = jnp.transpose(jnp.concatenate([a * inv for a in parts], axis=0))
    masks = head_mask((tok, 128))
    att = jnp.zeros((tok, 128), F32)
    for j in range(ny):
        f = [share_t[:, 8 * j + h : 8 * j + h + 1] for h in range(3)]
        factor = jnp.where(masks[0], f[0], jnp.where(masks[1], f[1], f[2]))
        att = att + factor * orecv[j].astype(F32)
    for t in range(nt):
        asend[t] = att[t * rows : (t + 1) * rows].astype(BF)

    def hand(i):
        to = (tp + i) % nt
        return rcopy(asend.at[to], arecv.at[tp], a_s.at[i - 1], a_r.at[i - 1], (sp, to))

    for i in range(1, nt):
        hand(i).start()
    arecv[tp] = asend[tp]
    share.finish()
    go(1)
    for i in range(1, nt):
        hand(i).wait_recv()

    full = jnp.concatenate([arecv[t] for t in range(nt)], axis=1)
    projected = jnp.dot(full, pw[...].reshape(nt * 128, d), preferred_element_type=F32)
    for c in load_r:
        c.wait()
    mixed = (res[...].astype(F32) + projected).astype(BF)
    wide = mixed.astype(F32)
    scale = lax.rsqrt(jnp.mean(wide * wide, axis=-1, keepdims=True) + 1e-6)
    half = y % 2
    feat[half, tp] = (wide * scale * gain[...]).astype(BF)
    partner = (z * ny + y + 1 - 2 * half, tp)
    near = Tp(nx, feat.at[half], f_xs.at[0], f_xr.at[0], f_ds.at[0], f_dr.at[0])
    far = Tp(nx, feat.at[1 - half], f_xs.at[1], f_xr.at[1], f_ds.at[1], f_dr.at[1])

    def across_y(which):
        return rcopy(feat.at[which, tp], feat.at[which, tp], f_s, f_r, partner)

    across_y(half).start()
    near.start()
    go(2)
    across_y(1 - half).wait_recv()
    far.start()
    go(2)
    for i in range(1, nx):
        near.forward(i)
    go(2)
    for i in range(1, nx):
        far.forward(i)
    go(len(todo))
    near.finish()
    far.finish()

    count = 2 * nt * rows
    ff = wbuf.shape[4]
    h = jnp.dot(feat[...].reshape(count, d), wbuf[:, :, 0].reshape(d, ff), preferred_element_type=F32)
    hidden[...] = jnp.square(jnp.maximum(h, 0.0)).astype(BF).reshape(2, nt * rows, ff)
    away = 1 - half

    def swap(g):
        return rcopy(psum.at[g], pair.at[g], pair_s.at[g], pair_r.at[g], (sp, other))

    for g in (away, half):
        total = nt_dot(hidden[g], wbuf[:, :, 1].reshape(d, ff))
        for t in range(nt):
            piece = total[t * rows : (t + 1) * rows]

            @pl.when(core == t % 2)
            def _():
                part[g, t // 2] = piece

            @pl.when(core != t % 2)
            def _():
                psum[g, t // 2] = piece.astype(BF)

        swap(g).start()

    def both(g, to):
        return part[g, to] + pair[g, to].astype(F32)

    opposite = nx // 2 if nx > 2 else 0
    direct = [i for i in range(1, nx) if i != opposite]

    def spare(which, i):
        to = (x + i) % nx
        return rcopy(
            xsend.at[which, i - 1],
            got.at[which, i - 1],
            g_s.at[which, i - 1],
            g_r.at[which, i - 1],
            (sp, to * 2 + core),
        )

    def over(j):
        return rcopy(ysend.at[j], yrecv.at[j], y_s.at[j], y_r.at[j], partner)

    swap(away).wait_recv()
    if opposite:
        ysend[1] = both(away, (x + opposite) % nx).astype(BF)
        over(1).start()
    for i in direct:
        xsend[0, i - 1] = both(away, (x + i) % nx).astype(BF)
        spare(0, i).start()
    swap(half).wait_recv()
    for i in direct:
        xsend[1, i - 1] = both(half, (x + i) % nx).astype(BF)
        spare(1, i).start()
    if opposite:
        over(1).wait_recv()
        xsend[1, opposite - 1] = (both(half, (x + opposite) % nx) + yrecv[1].astype(F32)).astype(BF)
        spare(1, opposite).start()
    acc = both(away, x)
    for i in direct:
        spare(0, i).wait_recv()
        acc = acc + got[0, i - 1].astype(F32)
    ysend[0] = acc.astype(BF)
    over(0).start()
    acc = wide + both(half, x)
    for i in direct:
        spare(1, i).wait_recv()
        acc = acc + got[1, i - 1].astype(F32)
    if opposite:
        spare(1, opposite).wait_recv()
        acc = acc + got[1, opposite - 1].astype(F32)
    over(0).wait_recv()
    out[...] = (acc + yrecv[0].astype(F32)).astype(BF)

    over(0).wait_send()
    if opposite:
        over(1).wait_send()
        spare(1, opposite).wait_send()
    for g in range(2):
        swap(g).wait_send()
    across_y(half).wait_send()
    for i in direct:
        for which in (0, 1):
            spare(which, i).wait_send()
    weights.finish()
    for chain in steps + steps_left:
        for c in chain:
            c.wait_send()
    for way in (0, 1):
        for s in range(1, q_last[way] + 1):
            q_ring(way, s, s - 1).wait_send()
    for i in range(1, ny):
        for c in give(i):
            c.wait_send()
    for i in range(1, nt):
        hand(i).wait_send()


def local(nz, ny, nt, *args):
    res, qn, kn, vn, qb, kb, vb, gn, gb, pn, pb, gain, up, down = args
    tok = qn.shape[0]
    rows, d = res.shape
    nx = nt // 2
    band, ff = up.shape

    dma = pltpu.SemaphoreType.DMA
    anyw = pl.BlockSpec(memory_space=pl.ANY)
    return pl.pallas_call(
        functools.partial(layer, nz, ny, nt),
        out_shape=jax.ShapeDtypeStruct((rows, d), BF),
        in_specs=[anyw] * 14,
        out_specs=pl.BlockSpec(memory_space=pltpu.VMEM),
        scratch_shapes=[
            pltpu.VMEM((6, 64, tok), BF),
            pltpu.VMEM((2, tok), F32),
            pltpu.VMEM((1, tok), F32),
            pltpu.VMEM((rows, d), BF),
            pltpu.VMEM((1, d), F32),
            pltpu.VMEM((2, band, ff), BF),
            pltpu.VMEM((nz, ny, 2, band, ff // 2), BF),
            pltpu.VMEM((ny, tok + 16, 128), BF),
            pltpu.VMEM((nz, tok, 128), BF),
            pltpu.VMEM((nz, tok, 256), BF),
            pltpu.VMEM((nz, 8, 256), F32),
            pltpu.VMEM((8, nz * tok), F32),
            pltpu.VMEM((nt, 128, d), BF),
            pltpu.VMEM((ny - 1, tok, 128), BF),
            pltpu.VMEM((ny - 1, 8, 256), F32),
            pltpu.VMEM((ny, tok, 128), BF),
            pltpu.VMEM((ny, 8, 256), F32),
            pltpu.VMEM((nt, rows, 128), BF),
            pltpu.VMEM((nt, rows, 128), BF),
            pltpu.VMEM((2, nt, rows, d), BF),
            pltpu.VMEM((2, nt * rows, ff // 2), BF),
            pltpu.VMEM((2, nx, rows, d), F32),
            pltpu.VMEM((2, nx, rows, d), BF),
            pltpu.VMEM((2, nx, rows, d), BF),
            pltpu.VMEM((2, nx - 1, rows, d), BF),
            pltpu.VMEM((2, nx - 1, rows, d), BF),
            pltpu.VMEM((2, rows, d), BF),
            pltpu.VMEM((2, rows, d), BF),
            dma((14,)),
            dma((2, ny // 2)),
            dma((2, ny // 2)),
            dma((3, nz - 1)),
            dma((3, nz - 1)),
            dma((nx - 1,)),
            dma((nx - 1,)),
            dma((nx,)),
            dma((nx,)),
            dma((2, ny - 1)),
            dma((2, ny - 1)),
            dma((nt - 1,)),
            dma((nt - 1,)),
            dma,
            dma,
            dma((2, nx - 1)),
            dma((2, nx - 1)),
            dma((2, nx)),
            dma((2, nx)),
            dma((ny // 2, 2)),
            dma((ny,)),
            dma((2, nz // 2, ny)),
            dma((2, nz // 2, ny)),
            dma((2,)),
            dma((2,)),
            dma((2, nx - 1)),
            dma((2, nx - 1)),
            dma((2,)),
            dma((2,)),
        ],
        compiler_params=pltpu.CompilerParams(
            collective_id=0, has_side_effects=True, vmem_limit_bytes=64 * 1024 * 1024 - 65536
        ),
        name="layer",
    )(qn.T, qb.T, kn.T, kb.T, vn.T, vb.T, gn.T, gb.T, pn, pb, res, gain.reshape(1, d), up, down.T)


def solution(mesh):
    nz, ny = split_sp(mesh)
    sp_tp = P("sp", "tp")
    return jax.shard_map(
        functools.partial(local, nz, ny, mesh.shape["tp"]),
        mesh=mesh,
        in_specs=(P(("sp", "tp"), None),)
        + (sp_tp,) * 8
        + (P("tp", None), P("tp", None), P(), sp_tp, P("tp", "sp")),
        out_specs=P(("sp", "tp"), None),
        check_vma=False,
    )
```

```python
import functools

import jax
import jax.numpy as jnp
from jax import lax
from jax.experimental import pallas as pl
from jax.experimental.pallas import tpu as pltpu
from jax.sharding import PartitionSpec as P

A_DIM = 32
B_DIM = 64
LOG2E = 1.4426950408889634
FAR = 1e30
MESH = pl.DeviceIdType.MESH
BF = jnp.bfloat16
F32 = jnp.float32


def split_sp(mesh):
    size = mesh.shape["sp"]
    ny = 1
    while ny * ny < size:
        ny *= 2
    return size // ny, ny


def rcopy(src, dst, send, recv, device):
    return pltpu.make_async_remote_copy(
        src_ref=src,
        dst_ref=dst,
        send_sem=send,
        recv_sem=recv,
        device_id=device,
        device_id_type=MESH,
    )


def nt_dot(a, b):
    return lax.dot_general(a, b, (((1,), (1,)), ((), ())), preferred_element_type=F32)


def head_mask(shape):
    lane = lax.broadcasted_iota(jnp.int32, shape, 1)
    return (lane < A_DIM, (lane >= A_DIM) & (lane < 2 * A_DIM), lane >= 2 * A_DIM)


SCALES = (A_DIM**-0.5 * LOG2E, A_DIM**-0.5 * LOG2E, B_DIM**-0.5 * LOG2E)


class Tp:
    def __init__(self, nx, buf, xs, xr, ds, dr):
        self.nx, self.buf, self.xs, self.xr, self.ds, self.dr = nx, buf, xs, xr, ds, dr
        self.sp, self.tp = lax.axis_index("sp"), lax.axis_index("tp")
        self.x, self.c = self.tp // 2, self.tp % 2

    def across(self, i):
        to = ((self.x + i) % self.nx) * 2 + self.c
        return rcopy(
            self.buf.at[self.tp], self.buf.at[self.tp], self.xs.at[i - 1], self.xr.at[i - 1], (self.sp, to)
        )

    def arrived(self, i):
        return ((self.x - i + self.nx) % self.nx) * 2 + self.c

    def beside(self, i):
        src = self.arrived(i)
        return rcopy(
            self.buf.at[src], self.buf.at[src], self.ds.at[i], self.dr.at[i], (self.sp, self.x * 2 + 1 - self.c)
        )

    def start(self):
        for i in range(1, self.nx):
            self.across(i).start()
        self.beside(0).start()

    def forward(self, i):
        self.across(i).wait_recv()
        self.beside(i).start()

    def finish(self):
        for i in range(self.nx):
            self.beside(i).wait_recv()
        for i in range(1, self.nx):
            self.across(i).wait_send()
        for i in range(self.nx):
            self.beside(i).wait_send()


class Weights:
    def __init__(self, nz, ny, src, buf, d_s, d_r, w_s, w_r):
        self.nz, self.ny, self.src, self.buf = nz, ny, src, buf
        self.d_s, self.d_r, self.w_s, self.w_r = d_s, d_r, w_s, w_r
        self.sp, self.tp = lax.axis_index("sp"), lax.axis_index("tp")
        self.z, self.y = self.sp // ny, self.sp % ny
        self.x, self.core = self.tp // 2, self.tp % 2
        self.width = buf.shape[4]
        self.mine = self.y % 2 == self.core
        self.last = nz // 2

    def half(self, c):
        return pl.ds(pl.multiple_of(c * self.width, self.width), self.width)

    def deal(self, t, c):
        to_y = ((self.y // 2 + t) % (self.ny // 2)) * 2 + self.core
        return rcopy(
            self.src.at[:, :, self.half(c)],
            self.buf.at[self.z, self.y],
            self.d_s.at[t, c],
            self.d_r.at[self.y],
            (self.z * self.ny + to_y, self.x * 2 + c),
        )

    def start(self):
        @pl.when(self.mine)
        def _():
            self.buf[self.z, self.y] = self.src[:, :, self.half(self.core)]

        @pl.when(jnp.logical_not(self.mine))
        def _():
            self.deal(0, self.core).start()

        self.deal(0, 1 - self.core).start()
        n = self.ny // 2
        self.later = []
        for t in range(1, n // 2 + 1):
            if 2 * t == n:
                self.later.append(t)
            else:
                self.later += [t + self.core * (n - 2 * t), n - t - self.core * (n - 2 * t)]
        self.deal_on()

    def deal_on(self):
        for t in self.later[:1]:
            for c in (0, 1):
                self.deal(t, c).start()
        del self.later[:1]

    def place(self, k):
        far = (k + 1) // 2
        return (self.y + far * (2 * (k % 2) - 1) + self.ny) % self.ny

    def copy(self, way, s, k, by):
        sign = 1 - 2 * way
        ref = self.buf.at[(self.z - sign * by + self.nz) % self.nz, self.place(k)]
        to = (self.z + sign + self.nz) % self.nz
        return rcopy(
            ref, ref, self.w_s.at[way, s - 1, k], self.w_r.at[way, s - 1, k], (to * self.ny + self.y, self.tp)
        )

    def ways(self, s, k):
        return (k % 2,) if s == self.last else (0, 1)

    def own_arrived(self, k):
        at = self.place(k)
        rcopy(
            self.src.at[:, :, self.half(self.core)],
            self.buf.at[self.z, at],
            self.d_s.at[0, 0],
            self.d_r.at[at],
            (self.sp, self.x * 2 + 1 - self.core),
        ).wait_recv()

    def own(self, k):
        if k == 0:
            pl.when(jnp.logical_not(self.mine))(lambda: self.own_arrived(k))
        else:
            self.own_arrived(k)
        for way in self.ways(1, k):
            self.copy(way, 1, k, 0).start()

    def own_inner(self, k):
        self.own_arrived(k)
        for way in (0, 1):

            @pl.when((self.last > 1) | (k % 2 == way))
            def _():
                self.copy(way, 1, k, 0).start()

    def tick(self, t):
        s, k = t // self.ny + 1, t % self.ny
        for way in self.ways(s, k):
            self.copy(way, s, k, s).wait_recv()
        if s < self.last:
            for way in self.ways(s + 1, k):
                self.copy(way, s + 1, k, s).start()

    def tick_inner(self, t):
        s, k = t // self.ny + 1, t % self.ny
        for way in (0, 1):
            self.copy(way, s, k, s).wait_recv()

            @pl.when((s + 1 < self.last) | (k % 2 == way))
            def _():
                self.copy(way, s + 1, k, s).start()

    def ticks(self):
        return self.last * self.ny

    def finish(self):
        @pl.when(jnp.logical_not(self.mine))
        def _():
            self.deal(0, self.core).wait_send()

        self.deal(0, 1 - self.core).wait_send()
        for t in range(1, self.ny // 2):
            for c in (0, 1):
                self.deal(t, c).wait_send()
        for s in range(1, self.last + 1):
            for k in range(self.ny):
                for way in self.ways(s, k):
                    self.copy(way, s, k, s - 1).wait_send()


def layer(
    nz,
    ny,
    nt,
    qn,
    qb,
    kn,
    kb,
    vn,
    vb,
    gn,
    gb,
    pn,
    pb,
    res_in,
    gain_in,
    up_in,
    down_in,
    out,
    raw,
    graw_n,
    graw_b,
    res,
    gain,
    wsrc,
    wbuf,
    qbuf,
    kbuf,
    vbuf,
    gbuf,
    gk,
    pw,
    osend,
    lsend,
    orecv,
    lrecv,
    asend,
    arecv,
    feat,
    hidden,
    part,
    psum,
    pair,
    xsend,
    got,
    ysend,
    yrecv,
    in_sem,
    q_s,
    q_r,
    kv_s,
    kv_r,
    pw_xs,
    pw_xr,
    pw_ds,
    pw_dr,
    p_s,
    p_r,
    a_s,
    a_r,
    f_s,
    f_r,
    f_xs,
    f_xr,
    f_ds,
    f_dr,
    d_s,
    d_r,
    w_s,
    w_r,
    pair_s,
    pair_r,
    g_s,
    g_r,
    y_s,
    y_r,
):
    nx = nt // 2
    sp, tp = lax.axis_index("sp"), lax.axis_index("tp")
    z, y = sp // ny, sp % ny
    x, core = tp // 2, tp % 2
    tok = qn.shape[1]
    rows, d = res.shape
    keys = nz * tok

    barrier = pltpu.get_barrier_semaphore()
    peers = [(z * ny + (y + i) % ny, tp) for i in range(1, ny)]
    up_z, down_z = ((z + 1) % nz) * ny + y, ((z + nz - 1) % nz) * ny + y
    other = x * 2 + 1 - core
    peers += [(z * ny + (y + i) % ny, other) for i in range(1, ny)]
    peers += [(up_z, tp), (down_z, tp)]
    peers += [(sp, (tp + i) % nt) for i in range(1, nt)]
    for peer in peers:
        pl.semaphore_signal(barrier, inc=1, device_id=peer, device_id_type=MESH)

    def load(i, src, dst):
        return pltpu.make_async_copy(src, dst, in_sem.at[i])

    loads = [load(i, r, raw.at[i]) for i, r in enumerate((qn, qb, kn, kb, vn, vb))]
    loads += [load(6, gn, graw_n), load(7, gb, graw_b)]
    load_w = [load(8, up_in, wsrc.at[0]), load(9, down_in, wsrc.at[1])]
    load_p = [load(10, pn, pw.at[tp, 0:64]), load(11, pb, pw.at[tp, 64:128])]
    load_r = [load(12, res_in, res), load(13, gain_in, gain)]
    for c in loads + load_w + load_p + load_r:
        c.start()

    for r in range(nz):
        vbuf[r, :, 128:256] = jnp.ones((tok, 128), BF)
    for c in loads:
        c.wait()

    qbuf[y, 0:tok, :] = jnp.transpose(raw[0:2].reshape(128, tok))
    kbuf[0] = jnp.transpose(raw[2:4].reshape(128, tok))
    vbuf[0, :, 0:128] = jnp.transpose(raw[4:6].reshape(128, tok))
    lane = lax.broadcasted_iota(jnp.int32, (tok, 128), 1)
    first_lane = lax.broadcasted_iota(jnp.int32, (16, 128), 1)
    starts = jnp.where(
        first_lane == 0,
        graw_n[0:1, 0:1],
        jnp.where(first_lane == 1, graw_n[1:2, 0:1], jnp.where(first_lane == 2, graw_b[0:1, 0:1], 0.0)),
    )
    qbuf[y, tok : tok + 16, :] = starts.astype(BF)
    gbuf[0] = jnp.zeros((8, 256), F32)
    gbuf[0, 0:2, 0:tok] = graw_n[...]
    gbuf[0, 2:3, 0:tok] = graw_b[...]

    for c in load_w + load_p:
        c.wait()
    pl.semaphore_wait(barrier, len(peers))

    weights = Weights(nz, ny, wsrc, wbuf, d_s, d_r, w_s, w_r)

    def ring(slot, src, to):
        return [
            rcopy(kbuf.at[src], kbuf.at[slot], kv_s.at[0, slot - 1], kv_r.at[0, slot - 1], (to, tp)),
            rcopy(
                vbuf.at[src, :, 0:128],
                vbuf.at[slot, :, 0:128],
                kv_s.at[1, slot - 1],
                kv_r.at[1, slot - 1],
                (to, tp),
            ),
            rcopy(gbuf.at[src], gbuf.at[slot], kv_s.at[2, slot - 1], kv_r.at[2, slot - 1], (to, tp)),
        ]

    rights = nz // 2
    lefts = nz - 1 - rights
    steps = [ring(s, s - 1, up_z) for s in range(1, rights + 1)]
    steps_left = [ring(nz - s, (nz - s + 1) % nz, down_z) for s in range(1, lefts + 1)]

    def q_ring(way, s, by):
        sign = 1 - 2 * way
        ref = qbuf.at[(y - sign * by + ny) % ny]
        return rcopy(
            ref, ref, q_s.at[way, s - 1], q_r.at[way, s - 1], (z * ny + (y + sign + ny) % ny, tp)
        )

    q_last = (ny // 2, ny - 1 - ny // 2)
    for kind in (2, 0, 1):
        for chain in steps[0:1] + steps_left[0:1]:
            chain[kind].start()
    for way in (0, 1):
        if q_last[way] > 0:
            q_ring(way, 1, 0).start()
    weights.start()
    share = Tp(nx, pw, pw_xs, pw_xr, pw_ds, pw_dr)
    share.start()

    most = max(rights, q_last[0])
    line = 0
    early = min(4, ny)
    for s in range(1, most + 1):
        for kind in (2, 0, 1):
            for chain, end in ((steps, rights), (steps_left, lefts)):
                if s <= end:
                    chain[s - 1][kind].wait_recv()
                    if s < end:
                        chain[s][kind].start()
            if kind == 0:
                for way in (0, 1):
                    if s <= q_last[way]:
                        q_ring(way, s, s).wait_recv()
                        if s < q_last[way]:
                            q_ring(way, s + 1, s).start()
        weights.deal_on()
        if line < early:
            weights.own(line)
            line += 1

    for r in range(nz):
        gk[:, r * tok : (r + 1) * tok] = jnp.where(r <= z, gbuf[r, :, 0:tok], FAR)

    col = lax.broadcasted_iota(jnp.int32, (1, keys), 1)

    def block(src, own, out_o, out_l):
        q = qbuf[src, 0:tok, :]
        masks = head_mask((tok, 128))
        k = kbuf[...].reshape(keys, 128)
        v = vbuf[...].reshape(keys, 256)
        outs, lses = [], []
        for h in range(3):
            s = nt_dot(jnp.where(masks[h], q, jnp.zeros_like(q)), k)
            ref = qbuf[src, tok : tok + 16, :][0:1, h : h + 1].astype(F32)
            bias = (ref - gk[h : h + 1, :]) * LOG2E
            if not own:
                bias = jnp.where((col < tok) & (y > src), -FAR, bias)
            s = s * SCALES[h] + bias
            if own:
                wide = min(keys, 256)
                first = s[:, 0:wide]
                at = lax.broadcasted_iota(jnp.int32, first.shape, 1)
                row = lax.broadcasted_iota(jnp.int32, first.shape, 0)
                first = jnp.where((at < tok) & (at > row), -FAR, first)
                s = jnp.concatenate([first, s[:, wide:]], axis=1) if keys > wide else first
            m = jnp.max(s, axis=1, keepdims=True)
            w = jnp.exp2(s - m).astype(BF)
            o = jnp.dot(w, v, preferred_element_type=F32)
            total = o[:, 128:256]
            outs.append(o[:, 0:128] / total)
            lses.append(m + jnp.log2(total))
        out_o[...] = jnp.where(masks[0], outs[0], jnp.where(masks[1], outs[1], outs[2])).astype(BF)
        lse = jnp.where(lane == 0, lses[0], jnp.where(lane == 1, lses[1], lses[2]))
        out_l[:, 0:tok] = jnp.transpose(lse)[0:8]

    def give(i):
        src = (y + ny - i) % ny
        to = (z * ny + src, tp)
        return [
            rcopy(osend.at[i - 1], orecv.at[y], p_s.at[0, i - 1], p_r.at[0, i - 1], to),
            rcopy(lsend.at[i - 1], lrecv.at[y], p_s.at[1, i - 1], p_r.at[1, i - 1], to),
        ]

    def one(i, carry):
        src = (y + ny - i) % ny
        block(src, False, osend.at[i - 1], lsend.at[i - 1])
        for c in give(i):
            c.start()
        return carry

    ticks = weights.ticks()
    inner = max(0, ticks - ny)
    per = min(1, inner // (ny - 1))

    def paced(i, carry):
        if early < ny:

            @pl.when(i <= ny - early)
            def _():
                weights.own_inner(i + early - 1)

        one(i, carry)
        for j in range(per):
            weights.tick_inner((i - 1) * per + j)
        return carry

    lax.fori_loop(1, ny, paced, 0)
    todo = list(range(per * (ny - 1), ticks))

    def go(count):
        for t in todo[:count]:
            weights.tick(t)
        del todo[:count]

    block(y, True, orecv.at[y], lrecv.at[y])
    for i in range(1, nx):
        share.forward(i)
    go(3)
    for i in range(1, ny):
        for c in give(i):
            c.wait_recv()

    go(4)

    lse = [lrecv[j, :, 0:tok] for j in range(ny)]
    peak = functools.reduce(jnp.maximum, lse)
    parts = [jnp.exp2(a - peak) for a in lse]
    inv = 1.0 / functools.reduce(jnp.add, parts)
    share_t = jnp.transpose(jnp.concatenate([a * inv for a in parts], axis=0))
    masks = head_mask((tok, 128))
    att = jnp.zeros((tok, 128), F32)
    for j in range(ny):
        f = [share_t[:, 8 * j + h : 8 * j + h + 1] for h in range(3)]
        factor = jnp.where(masks[0], f[0], jnp.where(masks[1], f[1], f[2]))
        att = att + factor * orecv[j].astype(F32)
    for t in range(nt):
        asend[t] = att[t * rows : (t + 1) * rows].astype(BF)

    def hand(i):
        to = (tp + i) % nt
        return rcopy(asend.at[to], arecv.at[tp], a_s.at[i - 1], a_r.at[i - 1], (sp, to))

    for i in range(1, nt):
        hand(i).start()
    arecv[tp] = asend[tp]
    go(3)
    share.finish()
    for i in range(1, nt):
        hand(i).wait_recv()

    full = jnp.concatenate([arecv[t] for t in range(nt)], axis=1)
    projected = jnp.dot(full, pw[...].reshape(nt * 128, d), preferred_element_type=F32)
    for c in load_r:
        c.wait()
    mixed = (res[...].astype(F32) + projected).astype(BF)
    wide = mixed.astype(F32)
    scale = lax.rsqrt(jnp.mean(wide * wide, axis=-1, keepdims=True) + 1e-6)
    half = y % 2
    feat[half, tp] = (wide * scale * gain[...]).astype(BF)
    partner = (z * ny + y + 1 - 2 * half, tp)
    near = Tp(nx, feat.at[half], f_xs.at[0], f_xr.at[0], f_ds.at[0], f_dr.at[0])
    far = Tp(nx, feat.at[1 - half], f_xs.at[1], f_xr.at[1], f_ds.at[1], f_dr.at[1])

    def across_y(which):
        return rcopy(feat.at[which, tp], feat.at[which, tp], f_s, f_r, partner)

    across_y(half).start()
    near.start()
    go(4)
    across_y(1 - half).wait_recv()
    far.start()
    go(3)
    for i in range(1, nx):
        near.forward(i)
    go(3)
    for i in range(1, nx):
        far.forward(i)
    go(len(todo))
    near.finish()
    far.finish()

    count = 2 * nt * rows
    ff = wbuf.shape[4]
    h = jnp.dot(feat[...].reshape(count, d), wbuf[:, :, 0].reshape(d, ff), preferred_element_type=F32)
    hidden[...] = jnp.square(jnp.maximum(h, 0.0)).astype(BF).reshape(2, nt * rows, ff)
    away = 1 - half

    def swap(g):
        return rcopy(psum.at[g], pair.at[g], pair_s.at[g], pair_r.at[g], (sp, other))

    for g in (away, half):
        total = nt_dot(hidden[g], wbuf[:, :, 1].reshape(d, ff))
        for t in range(nt):
            piece = total[t * rows : (t + 1) * rows]

            @pl.when(core == t % 2)
            def _():
                part[g, t // 2] = piece

            @pl.when(core != t % 2)
            def _():
                psum[g, t // 2] = piece.astype(BF)

        swap(g).start()

    def both(g, to):
        return part[g, to] + pair[g, to].astype(F32)

    opposite = nx // 2 if nx > 2 else 0
    direct = [i for i in range(1, nx) if i != opposite]

    def spare(which, i):
        to = (x + i) % nx
        return rcopy(
            xsend.at[which, i - 1],
            got.at[which, i - 1],
            g_s.at[which, i - 1],
            g_r.at[which, i - 1],
            (sp, to * 2 + core),
        )

    def over(j):
        return rcopy(ysend.at[j], yrecv.at[j], y_s.at[j], y_r.at[j], partner)

    swap(away).wait_recv()
    if opposite:
        ysend[1] = both(away, (x + opposite) % nx).astype(BF)
        over(1).start()
    for i in direct:
        xsend[0, i - 1] = both(away, (x + i) % nx).astype(BF)
        spare(0, i).start()
    swap(half).wait_recv()
    for i in direct:
        xsend[1, i - 1] = both(half, (x + i) % nx).astype(BF)
        spare(1, i).start()
    if opposite:
        over(1).wait_recv()
        xsend[1, opposite - 1] = (both(half, (x + opposite) % nx) + yrecv[1].astype(F32)).astype(BF)
        spare(1, opposite).start()
    acc = both(away, x)
    for i in direct:
        spare(0, i).wait_recv()
        acc = acc + got[0, i - 1].astype(F32)
    ysend[0] = acc.astype(BF)
    over(0).start()
    acc = wide + both(half, x)
    for i in direct:
        spare(1, i).wait_recv()
        acc = acc + got[1, i - 1].astype(F32)
    if opposite:
        spare(1, opposite).wait_recv()
        acc = acc + got[1, opposite - 1].astype(F32)
    over(0).wait_recv()
    out[...] = (acc + yrecv[0].astype(F32)).astype(BF)

    over(0).wait_send()
    if opposite:
        over(1).wait_send()
        spare(1, opposite).wait_send()
    for g in range(2):
        swap(g).wait_send()
    across_y(half).wait_send()
    for i in direct:
        for which in (0, 1):
            spare(which, i).wait_send()
    weights.finish()
    for chain in steps + steps_left:
        for c in chain:
            c.wait_send()
    for way in (0, 1):
        for s in range(1, q_last[way] + 1):
            q_ring(way, s, s - 1).wait_send()
    for i in range(1, ny):
        for c in give(i):
            c.wait_send()
    for i in range(1, nt):
        hand(i).wait_send()


def local(nz, ny, nt, *args):
    res, qn, kn, vn, qb, kb, vb, gn, gb, pn, pb, gain, up, down = args
    tok = qn.shape[0]
    rows, d = res.shape
    nx = nt // 2
    band, ff = up.shape

    dma = pltpu.SemaphoreType.DMA
    anyw = pl.BlockSpec(memory_space=pl.ANY)
    return pl.pallas_call(
        functools.partial(layer, nz, ny, nt),
        out_shape=jax.ShapeDtypeStruct((rows, d), BF),
        in_specs=[anyw] * 14,
        out_specs=pl.BlockSpec(memory_space=pltpu.VMEM),
        scratch_shapes=[
            pltpu.VMEM((6, 64, tok), BF),
            pltpu.VMEM((2, tok), F32),
            pltpu.VMEM((1, tok), F32),
            pltpu.VMEM((rows, d), BF),
            pltpu.VMEM((1, d), F32),
            pltpu.VMEM((2, band, ff), BF),
            pltpu.VMEM((nz, ny, 2, band, ff // 2), BF),
            pltpu.VMEM((ny, tok + 16, 128), BF),
            pltpu.VMEM((nz, tok, 128), BF),
            pltpu.VMEM((nz, tok, 256), BF),
            pltpu.VMEM((nz, 8, 256), F32),
            pltpu.VMEM((8, nz * tok), F32),
            pltpu.VMEM((nt, 128, d), BF),
            pltpu.VMEM((ny - 1, tok, 128), BF),
            pltpu.VMEM((ny - 1, 8, 256), F32),
            pltpu.VMEM((ny, tok, 128), BF),
            pltpu.VMEM((ny, 8, 256), F32),
            pltpu.VMEM((nt, rows, 128), BF),
            pltpu.VMEM((nt, rows, 128), BF),
            pltpu.VMEM((2, nt, rows, d), BF),
            pltpu.VMEM((2, nt * rows, ff // 2), BF),
            pltpu.VMEM((2, nx, rows, d), F32),
            pltpu.VMEM((2, nx, rows, d), BF),
            pltpu.VMEM((2, nx, rows, d), BF),
            pltpu.VMEM((2, nx - 1, rows, d), BF),
            pltpu.VMEM((2, nx - 1, rows, d), BF),
            pltpu.VMEM((2, rows, d), BF),
            pltpu.VMEM((2, rows, d), BF),
            dma((14,)),
            dma((2, ny // 2)),
            dma((2, ny // 2)),
            dma((3, nz - 1)),
            dma((3, nz - 1)),
            dma((nx - 1,)),
            dma((nx - 1,)),
            dma((nx,)),
            dma((nx,)),
            dma((2, ny - 1)),
            dma((2, ny - 1)),
            dma((nt - 1,)),
            dma((nt - 1,)),
            dma,
            dma,
            dma((2, nx - 1)),
            dma((2, nx - 1)),
            dma((2, nx)),
            dma((2, nx)),
            dma((ny // 2, 2)),
            dma((ny,)),
            dma((2, nz // 2, ny)),
            dma((2, nz // 2, ny)),
            dma((2,)),
            dma((2,)),
            dma((2, nx - 1)),
            dma((2, nx - 1)),
            dma((2,)),
            dma((2,)),
        ],
        compiler_params=pltpu.CompilerParams(
            collective_id=0, has_side_effects=True, vmem_limit_bytes=64 * 1024 * 1024 - 65536
        ),
        name="layer",
    )(qn.T, qb.T, kn.T, kb.T, vn.T, vb.T, gn.T, gb.T, pn, pb, res, gain.reshape(1, d), up, down.T)


def solution(mesh):
    nz, ny = split_sp(mesh)
    sp_tp = P("sp", "tp")
    return jax.shard_map(
        functools.partial(local, nz, ny, mesh.shape["tp"]),
        mesh=mesh,
        in_specs=(P(("sp", "tp"), None),)
        + (sp_tp,) * 8
        + (P("tp", None), P("tp", None), P(), sp_tp, P("tp", "sp")),
        out_specs=P(("sp", "tp"), None),
        check_vma=False,
    )
```

```python
import functools

import jax
import jax.numpy as jnp
from jax import lax
from jax.experimental import pallas as pl
from jax.experimental.pallas import tpu as pltpu
from jax.sharding import PartitionSpec as P

A_DIM = 32
B_DIM = 64
LOG2E = 1.4426950408889634
FAR = 1e30
MESH = pl.DeviceIdType.MESH
BF = jnp.bfloat16
F32 = jnp.float32


def split_sp(mesh):
    size = mesh.shape["sp"]
    ny = 1
    while ny * ny < size:
        ny *= 2
    return size // ny, ny


def rcopy(src, dst, send, recv, device):
    return pltpu.make_async_remote_copy(
        src_ref=src,
        dst_ref=dst,
        send_sem=send,
        recv_sem=recv,
        device_id=device,
        device_id_type=MESH,
    )


def nt_dot(a, b):
    return lax.dot_general(a, b, (((1,), (1,)), ((), ())), preferred_element_type=F32)


def head_mask(shape):
    lane = lax.broadcasted_iota(jnp.int32, shape, 1)
    return (lane < A_DIM, (lane >= A_DIM) & (lane < 2 * A_DIM), lane >= 2 * A_DIM)


SCALES = (A_DIM**-0.5 * LOG2E, A_DIM**-0.5 * LOG2E, B_DIM**-0.5 * LOG2E)


class Tp:
    def __init__(self, nx, buf, xs, xr, ds, dr):
        self.nx, self.buf, self.xs, self.xr, self.ds, self.dr = nx, buf, xs, xr, ds, dr
        self.sp, self.tp = lax.axis_index("sp"), lax.axis_index("tp")
        self.x, self.c = self.tp // 2, self.tp % 2

    def across(self, i):
        to = ((self.x + i) % self.nx) * 2 + self.c
        return rcopy(
            self.buf.at[self.tp], self.buf.at[self.tp], self.xs.at[i - 1], self.xr.at[i - 1], (self.sp, to)
        )

    def arrived(self, i):
        return ((self.x - i + self.nx) % self.nx) * 2 + self.c

    def beside(self, i):
        src = self.arrived(i)
        return rcopy(
            self.buf.at[src], self.buf.at[src], self.ds.at[i], self.dr.at[i], (self.sp, self.x * 2 + 1 - self.c)
        )

    def start(self):
        for i in range(1, self.nx):
            self.across(i).start()
        self.beside(0).start()

    def forward(self, i):
        self.across(i).wait_recv()
        self.beside(i).start()

    def finish(self):
        for i in range(self.nx):
            self.beside(i).wait_recv()
        for i in range(1, self.nx):
            self.across(i).wait_send()
        for i in range(self.nx):
            self.beside(i).wait_send()


class Weights:
    def __init__(self, nz, ny, src, buf, d_s, d_r, w_s, w_r):
        self.nz, self.ny, self.src, self.buf = nz, ny, src, buf
        self.d_s, self.d_r, self.w_s, self.w_r = d_s, d_r, w_s, w_r
        self.sp, self.tp = lax.axis_index("sp"), lax.axis_index("tp")
        self.z, self.y = self.sp // ny, self.sp % ny
        self.x, self.core = self.tp // 2, self.tp % 2
        self.width = buf.shape[4]
        self.mine = self.y % 2 == self.core
        self.last = nz // 2

    def half(self, c):
        return pl.ds(pl.multiple_of(c * self.width, self.width), self.width)

    def deal(self, t, c):
        to_y = ((self.y // 2 + t) % (self.ny // 2)) * 2 + self.core
        return rcopy(
            self.src.at[:, :, self.half(c)],
            self.buf.at[self.z, self.y],
            self.d_s.at[t, c],
            self.d_r.at[self.y],
            (self.z * self.ny + to_y, self.x * 2 + c),
        )

    def start(self):
        @pl.when(self.mine)
        def _():
            self.buf[self.z, self.y] = self.src[:, :, self.half(self.core)]

        @pl.when(jnp.logical_not(self.mine))
        def _():
            self.deal(0, self.core).start()

        self.deal(0, 1 - self.core).start()
        n = self.ny // 2
        self.later = []
        for t in range(1, n // 2 + 1):
            if 2 * t == n:
                self.later.append(t)
            else:
                self.later += [t + self.core * (n - 2 * t), n - t - self.core * (n - 2 * t)]
        self.deal_on()

    def deal_on(self):
        for t in self.later[:1]:
            for c in (0, 1):
                self.deal(t, c).start()
        del self.later[:1]

    def place(self, k):
        far = (k + 1) // 2
        return (self.y + far * (2 * (k % 2) - 1) + self.ny) % self.ny

    def copy(self, way, s, k, by):
        sign = 1 - 2 * way
        ref = self.buf.at[(self.z - sign * by + self.nz) % self.nz, self.place(k)]
        to = (self.z + sign + self.nz) % self.nz
        return rcopy(
            ref, ref, self.w_s.at[way, s - 1, k], self.w_r.at[way, s - 1, k], (to * self.ny + self.y, self.tp)
        )

    def ways(self, s, k):
        return (k % 2,) if s == self.last else (0, 1)

    def own_arrived(self, k):
        at = self.place(k)
        rcopy(
            self.src.at[:, :, self.half(self.core)],
            self.buf.at[self.z, at],
            self.d_s.at[0, 0],
            self.d_r.at[at],
            (self.sp, self.x * 2 + 1 - self.core),
        ).wait_recv()

    def own(self, k):
        if k == 0:
            pl.when(jnp.logical_not(self.mine))(lambda: self.own_arrived(k))
        else:
            self.own_arrived(k)
        for way in self.ways(1, k):
            self.copy(way, 1, k, 0).start()

    def own_inner(self, k):
        self.own_arrived(k)
        for way in (0, 1):

            @pl.when((self.last > 1) | (k % 2 == way))
            def _():
                self.copy(way, 1, k, 0).start()

    def tick(self, t):
        s, k = t // self.ny + 1, t % self.ny
        for way in self.ways(s, k):
            self.copy(way, s, k, s).wait_recv()
        if s < self.last:
            for way in self.ways(s + 1, k):
                self.copy(way, s + 1, k, s).start()

    def tick_inner(self, t):
        s, k = t // self.ny + 1, t % self.ny
        for way in (0, 1):
            self.copy(way, s, k, s).wait_recv()

            @pl.when((s + 1 < self.last) | (k % 2 == way))
            def _():
                self.copy(way, s + 1, k, s).start()

    def ticks(self):
        return self.last * self.ny

    def finish(self):
        @pl.when(jnp.logical_not(self.mine))
        def _():
            self.deal(0, self.core).wait_send()

        self.deal(0, 1 - self.core).wait_send()
        for t in range(1, self.ny // 2):
            for c in (0, 1):
                self.deal(t, c).wait_send()
        for s in range(1, self.last + 1):
            for k in range(self.ny):
                for way in self.ways(s, k):
                    self.copy(way, s, k, s - 1).wait_send()


def layer(
    nz,
    ny,
    nt,
    qn,
    qb,
    kn,
    kb,
    vn,
    vb,
    gn,
    gb,
    pn,
    pb,
    res_in,
    gain_in,
    up_in,
    down_in,
    out,
    raw,
    graw_n,
    graw_b,
    res,
    gain,
    wsrc,
    wbuf,
    qbuf,
    kbuf,
    vbuf,
    gbuf,
    gk,
    pw,
    osend,
    lsend,
    orecv,
    lrecv,
    asend,
    arecv,
    feat,
    hidden,
    part,
    psum,
    pair,
    xsend,
    got,
    ysend,
    yrecv,
    in_sem,
    q_s,
    q_r,
    kv_s,
    kv_r,
    pw_xs,
    pw_xr,
    pw_ds,
    pw_dr,
    p_s,
    p_r,
    a_s,
    a_r,
    f_s,
    f_r,
    f_xs,
    f_xr,
    f_ds,
    f_dr,
    d_s,
    d_r,
    w_s,
    w_r,
    pair_s,
    pair_r,
    g_s,
    g_r,
    y_s,
    y_r,
):
    nx = nt // 2
    sp, tp = lax.axis_index("sp"), lax.axis_index("tp")
    z, y = sp // ny, sp % ny
    x, core = tp // 2, tp % 2
    tok = qn.shape[1]
    rows, d = res.shape
    keys = nz * tok

    barrier = pltpu.get_barrier_semaphore()
    peers = [(z * ny + (y + i) % ny, tp) for i in range(1, ny)]
    up_z, down_z = ((z + 1) % nz) * ny + y, ((z + nz - 1) % nz) * ny + y
    other = x * 2 + 1 - core
    peers += [(z * ny + (y + i) % ny, other) for i in range(1, ny)]
    peers += [(up_z, tp), (down_z, tp)]
    peers += [(sp, (tp + i) % nt) for i in range(1, nt)]
    for peer in peers:
        pl.semaphore_signal(barrier, inc=1, device_id=peer, device_id_type=MESH)

    def load(i, src, dst):
        return pltpu.make_async_copy(src, dst, in_sem.at[i])

    loads = [load(i, r, raw.at[i]) for i, r in enumerate((qn, qb, kn, kb, vn, vb))]
    loads += [load(6, gn, graw_n), load(7, gb, graw_b)]
    load_w = [load(8, up_in, wsrc.at[0]), load(9, down_in, wsrc.at[1])]
    load_p = [load(10, pn, pw.at[tp, 0:64]), load(11, pb, pw.at[tp, 64:128])]
    load_r = [load(12, res_in, res), load(13, gain_in, gain)]
    for c in loads + load_w + load_p + load_r:
        c.start()

    for r in range(nz):
        vbuf[r, :, 128:256] = jnp.ones((tok, 128), BF)
    for c in loads:
        c.wait()

    qbuf[y, 0:tok, :] = jnp.transpose(raw[0:2].reshape(128, tok))
    kbuf[0] = jnp.transpose(raw[2:4].reshape(128, tok))
    vbuf[0, :, 0:128] = jnp.transpose(raw[4:6].reshape(128, tok))
    lane = lax.broadcasted_iota(jnp.int32, (tok, 128), 1)
    first_lane = lax.broadcasted_iota(jnp.int32, (16, 128), 1)
    starts = jnp.where(
        first_lane == 0,
        graw_n[0:1, 0:1],
        jnp.where(first_lane == 1, graw_n[1:2, 0:1], jnp.where(first_lane == 2, graw_b[0:1, 0:1], 0.0)),
    )
    qbuf[y, tok : tok + 16, :] = starts.astype(BF)
    gbuf[0] = jnp.zeros((8, 256), F32)
    gbuf[0, 0:2, 0:tok] = graw_n[...]
    gbuf[0, 2:3, 0:tok] = graw_b[...]

    for c in load_w + load_p:
        c.wait()
    pl.semaphore_wait(barrier, len(peers))

    weights = Weights(nz, ny, wsrc, wbuf, d_s, d_r, w_s, w_r)

    def ring(slot, src, to):
        return [
            rcopy(kbuf.at[src], kbuf.at[slot], kv_s.at[0, slot - 1], kv_r.at[0, slot - 1], (to, tp)),
            rcopy(
                vbuf.at[src, :, 0:128],
                vbuf.at[slot, :, 0:128],
                kv_s.at[1, slot - 1],
                kv_r.at[1, slot - 1],
                (to, tp),
            ),
            rcopy(gbuf.at[src], gbuf.at[slot], kv_s.at[2, slot - 1], kv_r.at[2, slot - 1], (to, tp)),
        ]

    rights = nz // 2
    lefts = nz - 1 - rights
    steps = [ring(s, s - 1, up_z) for s in range(1, rights + 1)]
    steps_left = [ring(nz - s, (nz - s + 1) % nz, down_z) for s in range(1, lefts + 1)]

    def q_ring(way, s, by):
        sign = 1 - 2 * way
        ref = qbuf.at[(y - sign * by + ny) % ny]
        return rcopy(
            ref, ref, q_s.at[way, s - 1], q_r.at[way, s - 1], (z * ny + (y + sign + ny) % ny, tp)
        )

    q_last = (ny // 2, ny - 1 - ny // 2)
    for kind in (2, 0, 1):
        for chain in steps[0:1] + steps_left[0:1]:
            chain[kind].start()
    for way in (0, 1):
        if q_last[way] > 0:
            q_ring(way, 1, 0).start()
    weights.start()
    share = Tp(nx, pw, pw_xs, pw_xr, pw_ds, pw_dr)
    share.start()

    most = max(rights, q_last[0])
    line = 0
    early = min(4, ny)
    weights.own(0)
    line = 1
    for s in range(1, most + 1):
        for kind in (2, 0, 1):
            for chain, end in ((steps, rights), (steps_left, lefts)):
                if s <= end:
                    chain[s - 1][kind].wait_recv()
                    if s < end:
                        chain[s][kind].start()
            if kind == 0:
                for way in (0, 1):
                    if s <= q_last[way]:
                        q_ring(way, s, s).wait_recv()
                        if s < q_last[way]:
                            q_ring(way, s + 1, s).start()
        weights.deal_on()
        if line < early:
            weights.own(line)
            line += 1

    for r in range(nz):
        gk[:, r * tok : (r + 1) * tok] = jnp.where(r <= z, gbuf[r, :, 0:tok], FAR)

    col = lax.broadcasted_iota(jnp.int32, (1, keys), 1)

    def block(src, own, out_o, out_l):
        q = qbuf[src, 0:tok, :]
        masks = head_mask((tok, 128))
        k = kbuf[...].reshape(keys, 128)
        v = vbuf[...].reshape(keys, 256)
        outs, lses = [], []
        for h in range(3):
            s = nt_dot(jnp.where(masks[h], q, jnp.zeros_like(q)), k)
            ref = qbuf[src, tok : tok + 16, :][0:1, h : h + 1].astype(F32)
            bias = (ref - gk[h : h + 1, :]) * LOG2E
            if not own:
                bias = jnp.where((col < tok) & (y > src), -FAR, bias)
            s = s * SCALES[h] + bias
            if own:
                wide = min(keys, 256)
                first = s[:, 0:wide]
                at = lax.broadcasted_iota(jnp.int32, first.shape, 1)
                row = lax.broadcasted_iota(jnp.int32, first.shape, 0)
                first = jnp.where((at < tok) & (at > row), -FAR, first)
                s = jnp.concatenate([first, s[:, wide:]], axis=1) if keys > wide else first
            m = jnp.max(s, axis=1, keepdims=True)
            w = jnp.exp2(s - m).astype(BF)
            o = jnp.dot(w, v, preferred_element_type=F32)
            total = o[:, 128:256]
            outs.append(o[:, 0:128] / total)
            lses.append(m + jnp.log2(total))
        out_o[...] = jnp.where(masks[0], outs[0], jnp.where(masks[1], outs[1], outs[2])).astype(BF)
        lse = jnp.where(lane == 0, lses[0], jnp.where(lane == 1, lses[1], lses[2]))
        out_l[:, 0:tok] = jnp.transpose(lse)[0:8]

    def give(i):
        src = (y + ny - i) % ny
        to = (z * ny + src, tp)
        return [
            rcopy(osend.at[i - 1], orecv.at[y], p_s.at[0, i - 1], p_r.at[0, i - 1], to),
            rcopy(lsend.at[i - 1], lrecv.at[y], p_s.at[1, i - 1], p_r.at[1, i - 1], to),
        ]

    def one(i, carry):
        src = (y + ny - i) % ny
        block(src, False, osend.at[i - 1], lsend.at[i - 1])
        for c in give(i):
            c.start()
        return carry

    ticks = weights.ticks()
    inner = max(0, ticks - ny)
    per = min(1, inner // (ny - 1))

    def paced(i, carry):
        if early < ny:

            @pl.when(i <= ny - early)
            def _():
                weights.own_inner(i + early - 1)

        one(i, carry)
        for j in range(per):
            weights.tick_inner((i - 1) * per + j)
        return carry

    lax.fori_loop(1, ny, paced, 0)
    todo = list(range(per * (ny - 1), ticks))

    def go(count):
        for t in todo[:count]:
            weights.tick(t)
        del todo[:count]

    block(y, True, orecv.at[y], lrecv.at[y])
    for i in range(1, nx):
        share.forward(i)
    go(3)
    for i in range(1, ny):
        for c in give(i):
            c.wait_recv()

    go(4)

    lse = [lrecv[j, :, 0:tok] for j in range(ny)]
    peak = functools.reduce(jnp.maximum, lse)
    parts = [jnp.exp2(a - peak) for a in lse]
    inv = 1.0 / functools.reduce(jnp.add, parts)
    share_t = jnp.transpose(jnp.concatenate([a * inv for a in parts], axis=0))
    masks = head_mask((tok, 128))
    att = jnp.zeros((tok, 128), F32)
    for j in range(ny):
        f = [share_t[:, 8 * j + h : 8 * j + h + 1] for h in range(3)]
        factor = jnp.where(masks[0], f[0], jnp.where(masks[1], f[1], f[2]))
        att = att + factor * orecv[j].astype(F32)
    for t in range(nt):
        asend[t] = att[t * rows : (t + 1) * rows].astype(BF)

    def hand(i):
        to = (tp + i) % nt
        return rcopy(asend.at[to], arecv.at[tp], a_s.at[i - 1], a_r.at[i - 1], (sp, to))

    for i in range(1, nt):
        hand(i).start()
    arecv[tp] = asend[tp]
    go(3)
    share.finish()
    for i in range(1, nt):
        hand(i).wait_recv()

    full = jnp.concatenate([arecv[t] for t in range(nt)], axis=1)
    projected = jnp.dot(full, pw[...].reshape(nt * 128, d), preferred_element_type=F32)
    for c in load_r:
        c.wait()
    mixed = (res[...].astype(F32) + projected).astype(BF)
    wide = mixed.astype(F32)
    scale = lax.rsqrt(jnp.mean(wide * wide, axis=-1, keepdims=True) + 1e-6)
    half = y % 2
    feat[half, tp] = (wide * scale * gain[...]).astype(BF)
    partner = (z * ny + y + 1 - 2 * half, tp)
    near = Tp(nx, feat.at[half], f_xs.at[0], f_xr.at[0], f_ds.at[0], f_dr.at[0])
    far = Tp(nx, feat.at[1 - half], f_xs.at[1], f_xr.at[1], f_ds.at[1], f_dr.at[1])

    def across_y(which):
        return rcopy(feat.at[which, tp], feat.at[which, tp], f_s, f_r, partner)

    across_y(half).start()
    near.start()
    go(4)
    across_y(1 - half).wait_recv()
    far.start()
    go(3)
    for i in range(1, nx):
        near.forward(i)
    go(3)
    for i in range(1, nx):
        far.forward(i)
    go(len(todo))
    near.finish()
    far.finish()

    count = 2 * nt * rows
    ff = wbuf.shape[4]
    h = jnp.dot(feat[...].reshape(count, d), wbuf[:, :, 0].reshape(d, ff), preferred_element_type=F32)
    hidden[...] = jnp.square(jnp.maximum(h, 0.0)).astype(BF).reshape(2, nt * rows, ff)
    away = 1 - half

    def swap(g):
        return rcopy(psum.at[g], pair.at[g], pair_s.at[g], pair_r.at[g], (sp, other))

    for g in (away, half):
        total = nt_dot(hidden[g], wbuf[:, :, 1].reshape(d, ff))
        for t in range(nt):
            piece = total[t * rows : (t + 1) * rows]

            @pl.when(core == t % 2)
            def _():
                part[g, t // 2] = piece

            @pl.when(core != t % 2)
            def _():
                psum[g, t // 2] = piece.astype(BF)

        swap(g).start()

    def both(g, to):
        return part[g, to] + pair[g, to].astype(F32)

    opposite = nx // 2 if nx > 2 else 0
    direct = [i for i in range(1, nx) if i != opposite]

    def spare(which, i):
        to = (x + i) % nx
        return rcopy(
            xsend.at[which, i - 1],
            got.at[which, i - 1],
            g_s.at[which, i - 1],
            g_r.at[which, i - 1],
            (sp, to * 2 + core),
        )

    def over(j):
        return rcopy(ysend.at[j], yrecv.at[j], y_s.at[j], y_r.at[j], partner)

    swap(away).wait_recv()
    if opposite:
        ysend[1] = both(away, (x + opposite) % nx).astype(BF)
        over(1).start()
    for i in direct:
        xsend[0, i - 1] = both(away, (x + i) % nx).astype(BF)
        spare(0, i).start()
    swap(half).wait_recv()
    for i in direct:
        xsend[1, i - 1] = both(half, (x + i) % nx).astype(BF)
        spare(1, i).start()
    if opposite:
        over(1).wait_recv()
        xsend[1, opposite - 1] = (both(half, (x + opposite) % nx) + yrecv[1].astype(F32)).astype(BF)
        spare(1, opposite).start()
    acc = both(away, x)
    for i in direct:
        spare(0, i).wait_recv()
        acc = acc + got[0, i - 1].astype(F32)
    ysend[0] = acc.astype(BF)
    over(0).start()
    acc = wide + both(half, x)
    for i in direct:
        spare(1, i).wait_recv()
        acc = acc + got[1, i - 1].astype(F32)
    if opposite:
        spare(1, opposite).wait_recv()
        acc = acc + got[1, opposite - 1].astype(F32)
    over(0).wait_recv()
    out[...] = (acc + yrecv[0].astype(F32)).astype(BF)

    over(0).wait_send()
    if opposite:
        over(1).wait_send()
        spare(1, opposite).wait_send()
    for g in range(2):
        swap(g).wait_send()
    across_y(half).wait_send()
    for i in direct:
        for which in (0, 1):
            spare(which, i).wait_send()
    weights.finish()
    for chain in steps + steps_left:
        for c in chain:
            c.wait_send()
    for way in (0, 1):
        for s in range(1, q_last[way] + 1):
            q_ring(way, s, s - 1).wait_send()
    for i in range(1, ny):
        for c in give(i):
            c.wait_send()
    for i in range(1, nt):
        hand(i).wait_send()


def local(nz, ny, nt, *args):
    res, qn, kn, vn, qb, kb, vb, gn, gb, pn, pb, gain, up, down = args
    tok = qn.shape[0]
    rows, d = res.shape
    nx = nt // 2
    band, ff = up.shape

    dma = pltpu.SemaphoreType.DMA
    anyw = pl.BlockSpec(memory_space=pl.ANY)
    return pl.pallas_call(
        functools.partial(layer, nz, ny, nt),
        out_shape=jax.ShapeDtypeStruct((rows, d), BF),
        in_specs=[anyw] * 14,
        out_specs=pl.BlockSpec(memory_space=pltpu.VMEM),
        scratch_shapes=[
            pltpu.VMEM((6, 64, tok), BF),
            pltpu.VMEM((2, tok), F32),
            pltpu.VMEM((1, tok), F32),
            pltpu.VMEM((rows, d), BF),
            pltpu.VMEM((1, d), F32),
            pltpu.VMEM((2, band, ff), BF),
            pltpu.VMEM((nz, ny, 2, band, ff // 2), BF),
            pltpu.VMEM((ny, tok + 16, 128), BF),
            pltpu.VMEM((nz, tok, 128), BF),
            pltpu.VMEM((nz, tok, 256), BF),
            pltpu.VMEM((nz, 8, 256), F32),
            pltpu.VMEM((8, nz * tok), F32),
            pltpu.VMEM((nt, 128, d), BF),
            pltpu.VMEM((ny - 1, tok, 128), BF),
            pltpu.VMEM((ny - 1, 8, 256), F32),
            pltpu.VMEM((ny, tok, 128), BF),
            pltpu.VMEM((ny, 8, 256), F32),
            pltpu.VMEM((nt, rows, 128), BF),
            pltpu.VMEM((nt, rows, 128), BF),
            pltpu.VMEM((2, nt, rows, d), BF),
            pltpu.VMEM((2, nt * rows, ff // 2), BF),
            pltpu.VMEM((2, nx, rows, d), F32),
            pltpu.VMEM((2, nx, rows, d), BF),
            pltpu.VMEM((2, nx, rows, d), BF),
            pltpu.VMEM((2, nx - 1, rows, d), BF),
            pltpu.VMEM((2, nx - 1, rows, d), BF),
            pltpu.VMEM((2, rows, d), BF),
            pltpu.VMEM((2, rows, d), BF),
            dma((14,)),
            dma((2, ny // 2)),
            dma((2, ny // 2)),
            dma((3, nz - 1)),
            dma((3, nz - 1)),
            dma((nx - 1,)),
            dma((nx - 1,)),
            dma((nx,)),
            dma((nx,)),
            dma((2, ny - 1)),
            dma((2, ny - 1)),
            dma((nt - 1,)),
            dma((nt - 1,)),
            dma,
            dma,
            dma((2, nx - 1)),
            dma((2, nx - 1)),
            dma((2, nx)),
            dma((2, nx)),
            dma((ny // 2, 2)),
            dma((ny,)),
            dma((2, nz // 2, ny)),
            dma((2, nz // 2, ny)),
            dma((2,)),
            dma((2,)),
            dma((2, nx - 1)),
            dma((2, nx - 1)),
            dma((2,)),
            dma((2,)),
        ],
        compiler_params=pltpu.CompilerParams(
            collective_id=0, has_side_effects=True, vmem_limit_bytes=64 * 1024 * 1024 - 65536
        ),
        name="layer",
    )(qn.T, qb.T, kn.T, kb.T, vn.T, vb.T, gn.T, gb.T, pn, pb, res, gain.reshape(1, d), up, down.T)


def solution(mesh):
    nz, ny = split_sp(mesh)
    sp_tp = P("sp", "tp")
    return jax.shard_map(
        functools.partial(local, nz, ny, mesh.shape["tp"]),
        mesh=mesh,
        in_specs=(P(("sp", "tp"), None),)
        + (sp_tp,) * 8
        + (P("tp", None), P("tp", None), P(), sp_tp, P("tp", "sp")),
        out_specs=P(("sp", "tp"), None),
        check_vma=False,
    )
```
